32 devices in a mesh: grp: 2 (over y), sp: 4 (over z), tp: 4 (over x, core).
Axes of the slice: x: 2, y: 2, z: 4, core: 2. Of those that a mesh axis runs over, the one named last changes fastest.
Arguments:
- queries: bfloat16 [6144, 1024], P(('grp', 'sp'), 'tp'), parts along dimension 0, may hold values from -160 to 160
- key_rows: bfloat16 [6144, 256], P(('grp', 'sp'), 'tp'), parts along dimension 0, may hold values from -4 to 4
- value_rows: bfloat16 [6144, 256], P(('grp', 'sp'), 'tp'), parts along dimension 0, may hold values from -5 to 5
- sink_logits: float32 [16], P('tp'), may hold values from 2 to 6
- out_weight: bfloat16 [1024, 2048], replicated, may hold values from -0.75 to 0.75
- residual: bfloat16 [6144, 2048], P(('grp', 'sp', 'tp')), parts along dimension 0, may hold values from -6 to 6
- norm_gain: float32 [2048], replicated, may hold values from 0.1 to 1.9
- up_weight: bfloat16 [2048, 4096], P('sp', 'tp'), may hold values from -0.125 to 0.125
- down_weight: bfloat16 [4096, 2048], P('tp', 'sp'), may hold values from -0.09375 to 0.09375
Outputs:
- layer_out: bfloat16 [6144, 2048], P(('grp', 'sp', 'tp')), parts along dimension 0
The draws below stay inside these ranges and needn't reach their ends.
There are 2 independent parts, one for each index of `grp`. The reference program is written for one: setup_inputs(seed, part) draws one part's arguments, and reference() takes and returns one part's arrays. A program takes and returns all parts, laid end to end along the dimension named above; an argument that names none is the same for every part. Nothing has to cross between parts.
All inputs are finite; a program needn't handle non-finite values.
Results may differ from the reference program's by a relative error of at most 0.017.
Values may be sent and summed in bfloat16 or wider, within the bound.
A program may use at most 64 MiB of HBM per device.

```python
import jax
import jax.numpy as jnp
from jax import lax

D = 2048
Q_HEADS = 16
KV_HEADS = 4
HEAD_DIM = 64
FF = 4096
WINDOW = 128
TOKENS = 3072
N_TP = 4


def attention_base(key):
    query_key = jax.random.fold_in(key, 11)
    row_key = jax.random.fold_in(key, 12)
    keys_raw = jax.random.truncated_normal(row_key, -4.0, 4.0, (TOKENS, KV_HEADS, HEAD_DIM), jnp.float32)
    queries_raw = jax.random.truncated_normal(query_key, -4.0, 4.0, (TOKENS, Q_HEADS, HEAD_DIM), jnp.float32)
    return (queries_raw, keys_raw)


def draw_queries(key, part):
    return attention_base(key)[0].reshape(TOKENS, Q_HEADS * HEAD_DIM).astype(jnp.bfloat16)


def draw_key_rows(key, part):
    return attention_base(key)[1].reshape(TOKENS, KV_HEADS * HEAD_DIM).astype(jnp.bfloat16)


def shard_levels(own_key, dims, cuts, least, largest):
    gain = 1.0
    for axis_at, blocks in cuts:
        heights = jax.random.uniform(jax.random.fold_in(jax.random.fold_in(own_key, 6), axis_at), (blocks,), jnp.float32, least / len(cuts), largest / len(cuts))
        gain = gain * jnp.repeat(jnp.exp(heights), dims[axis_at] // blocks).reshape((-1,) + (1,) * (len(dims) - 1 - axis_at))
    return gain


def scatter_about(own_key, dims, scale, bound, shards=(), kind=jnp.bfloat16):
    entries = jax.random.normal(own_key, dims, jnp.float32) * scale
    if len(shards) > 0:
        entries = shard_levels(own_key, dims, shards, -0.22, 0.18) * entries
    return jnp.clip(entries, min=-bound, max=bound).astype(kind)


def setup_inputs(seed: int = 0, part: int = 0) -> dict:
    streams_of = jax.random.split(jax.random.key(seed), 10)
    own_keys = jax.random.split(jax.random.fold_in(streams_of[9], part), 10)
    queries = draw_queries(jax.random.fold_in(jax.random.fold_in(streams_of[9], part), 71), part)
    key_rows = draw_key_rows(jax.random.fold_in(jax.random.fold_in(streams_of[9], part), 71), part)
    value_rows = scatter_about(own_keys[2], (TOKENS, KV_HEADS * HEAD_DIM), 1.0, 5.0, ((0, 4), (1, 4)))
    sink_logits = jnp.clip(2.0 + 4.0 * jax.random.uniform(streams_of[3], (Q_HEADS,), jnp.float32) ** shard_levels(streams_of[3], (Q_HEADS,), ((0, 4),), -0.2, 0.2), 2.0, 6.0)
    out_weight = scatter_about(streams_of[4], (Q_HEADS * HEAD_DIM, D), (Q_HEADS * HEAD_DIM // 16) ** -0.5, 0.75)
    residual = scatter_about(own_keys[5], (TOKENS, D), 1.0, 6.0, ((0, 16),))
    norm_gain = jnp.clip(1.0 + 0.18 * jax.random.normal(streams_of[6], (D,), jnp.float32), 0.1, 1.9)
    up_weight = scatter_about(streams_of[7], (D, FF), D ** -0.5, 0.125, ((0, 4), (1, 4)))
    down_weight = scatter_about(streams_of[8], (FF, D), FF ** -0.5, 0.09375, ((0, 4), (1, 4)))
    return {"queries": queries, "key_rows": key_rows, "value_rows": value_rows, "sink_logits": sink_logits, "out_weight": out_weight, "residual": residual, "norm_gain": norm_gain, "up_weight": up_weight, "down_weight": down_weight}


def band_attend(queries, key_rows, value_rows, sink_logits):
    rows = queries.shape[0]
    group = queries.shape[1] // HEAD_DIM
    blocks = rows // WINDOW
    zero_tail = jnp.zeros((WINDOW, HEAD_DIM), jnp.float32)
    all_keys = jnp.concatenate([zero_tail, key_rows.astype(jnp.float32)], axis=0).reshape(blocks + 1, WINDOW, HEAD_DIM)
    all_values = jnp.concatenate([zero_tail, value_rows.astype(jnp.float32)], axis=0).reshape(blocks + 1, WINDOW, HEAD_DIM)
    key_blocks = jnp.concatenate([all_keys[:-1], all_keys[1:]], axis=1)
    value_blocks = jnp.concatenate([all_values[:-1], all_values[1:]], axis=1)
    query_blocks = queries.astype(jnp.float32).reshape(blocks, WINDOW, group, HEAD_DIM)
    scores = jnp.einsum('nqgd,nsd->ngqs', query_blocks, key_blocks) * HEAD_DIM ** (-0.5)
    q_local = jnp.arange(WINDOW, dtype=jnp.int32) + WINDOW
    k_local = jnp.arange(2 * WINDOW, dtype=jnp.int32)
    distance = q_local[:, None] - k_local[None, :]
    key_position = (jnp.arange(blocks, dtype=jnp.int32)[:, None] - 1) * WINDOW + k_local[None, :]
    valid = ((distance >= 0) & (distance < WINDOW))[None] & (key_position >= 0)[:, None, :]
    scores = jnp.where(valid[:, None], scores, -1e+30)
    sink = sink_logits.astype(jnp.float32)[None, :, None, None]
    top = jnp.maximum(lax.optimization_barrier(jnp.max(scores, axis=-1, keepdims=True)), sink)
    weights = jnp.exp(scores - top)
    total = lax.optimization_barrier(jnp.sum(weights, axis=-1, keepdims=True)) + jnp.exp(sink - top)
    probs = (weights / total).astype(jnp.bfloat16).astype(jnp.float32)
    result = jnp.einsum('ngqs,nsd->nqgd', probs, value_blocks)
    return result.astype(jnp.bfloat16).reshape(rows, group * HEAD_DIM)

def reference(queries, key_rows, value_rows, sink_logits, out_weight, residual, norm_gain, up_weight, down_weight):
    group = Q_HEADS // KV_HEADS
    pieces = []
    for head in range(KV_HEADS):
        pieces.append(band_attend(queries[:, head * group * HEAD_DIM:(head + 1) * group * HEAD_DIM], key_rows[:, head * HEAD_DIM:(head + 1) * HEAD_DIM], value_rows[:, head * HEAD_DIM:(head + 1) * HEAD_DIM], sink_logits[head * group:(head + 1) * group]))
    attended = jnp.concatenate(pieces, axis=1)
    projected = jnp.dot(attended, out_weight, preferred_element_type=jnp.float32)
    mixed = (residual.astype(jnp.float32) + projected).astype(jnp.bfloat16)
    mixed32 = mixed.astype(jnp.float32)
    scale = lax.rsqrt(lax.optimization_barrier(jnp.mean(mixed32 * mixed32, axis=-1, keepdims=True)) + 1e-06)
    normed = (mixed32 * scale * norm_gain).astype(jnp.bfloat16)
    hidden = jnp.square(jax.nn.relu(jnp.dot(normed, up_weight, preferred_element_type=jnp.float32))).astype(jnp.bfloat16)
    width = FF // N_TP
    down = jnp.zeros((TOKENS, D), jnp.float32)
    for index in range(N_TP):
        partial_product = jnp.dot(hidden[:, index * width:(index + 1) * width], down_weight[index * width:(index + 1) * width], preferred_element_type=jnp.float32).astype(jnp.bfloat16)
        down = down + lax.optimization_barrier(partial_product).astype(jnp.float32)
    return (mixed32 + down).astype(jnp.bfloat16)
```

```python
import functools

import jax
import jax.numpy as jnp
from jax import lax
from jax.experimental import pallas as pl
from jax.experimental.pallas import tpu as pltpu
from jax.sharding import PartitionSpec as P

HEAD_DIM = 64
WINDOW = 128


def shifted(value, axis, steps):
    count = lax.axis_size(axis)
    leading, last = (max(0, -steps), min(count, count - steps))
    return lax.ppermute(value, axis, [(source, source + steps) for source in range(leading, last)])


def band_attend(queries, key_rows, value_rows, sink_logits, tail_keys, tail_values, offset):
    rows = queries.shape[0]
    kv_heads = key_rows.shape[1] // HEAD_DIM
    group = queries.shape[1] // (kv_heads * HEAD_DIM)
    blocks = rows // WINDOW
    all_keys = jnp.concatenate([tail_keys, key_rows], axis=0).reshape(
        blocks + 1, WINDOW, kv_heads, HEAD_DIM
    )
    all_values = jnp.concatenate([tail_values, value_rows], axis=0).reshape(
        blocks + 1, WINDOW, kv_heads, HEAD_DIM
    )
    key_blocks = jnp.concatenate([all_keys[:-1], all_keys[1:]], axis=1)
    value_blocks = jnp.concatenate([all_values[:-1], all_values[1:]], axis=1)
    query_blocks = queries.reshape(blocks, WINDOW, kv_heads, group, HEAD_DIM)
    scores = jnp.einsum(
        "nqkgd,nskd->nkgqs", query_blocks, key_blocks, preferred_element_type=jnp.float32
    ) * HEAD_DIM ** (-0.5)
    q_local = jnp.arange(WINDOW, dtype=jnp.int32) + WINDOW
    k_local = jnp.arange(2 * WINDOW, dtype=jnp.int32)
    distance = q_local[:, None] - k_local[None, :]
    key_position = (
        offset + (jnp.arange(blocks, dtype=jnp.int32)[:, None] - 1) * WINDOW + k_local[None, :]
    )
    valid = ((distance >= 0) & (distance < WINDOW))[None] & (key_position >= 0)[:, None, :]
    scores = jnp.where(valid[:, None, None], scores, -1e30)
    sink = sink_logits.reshape(kv_heads, group)[None, :, :, None, None]
    top = jnp.maximum(jnp.max(scores, axis=-1, keepdims=True), sink)
    weights = jnp.exp(scores - top)
    total = jnp.sum(weights, axis=-1, keepdims=True) + jnp.exp(sink - top)
    probs = (weights / total).astype(jnp.bfloat16)
    result = jnp.einsum(
        "nkgqs,nskd->nqkgd", probs, value_blocks, preferred_element_type=jnp.float32
    )
    return result.astype(jnp.bfloat16).reshape(rows, kv_heads * group * HEAD_DIM)


def body(
    queries,
    key_rows,
    value_rows,
    sink_logits,
    out_weight,
    residual,
    norm_gain,
    up_weight,
    down_weight,
):
    rows = queries.shape[0]
    width = key_rows.shape[1]
    kv_pair = jnp.concatenate([key_rows[rows - WINDOW :], value_rows[rows - WINDOW :]], axis=1)
    tail = shifted(kv_pair, "sp", 1)
    offset = lax.axis_index("sp") * rows
    attended = band_attend(
        queries, key_rows, value_rows, sink_logits, tail[:, :width], tail[:, width:], offset
    )
    head_cols = attended.shape[1]
    own_rows = lax.dynamic_slice_in_dim(out_weight, lax.axis_index("tp") * head_cols, head_cols, 0)
    projected = lax.psum_scatter(
        jnp.dot(attended, own_rows, preferred_element_type=jnp.float32).astype(jnp.bfloat16),
        "tp",
        scatter_dimension=0,
        tiled=True,
    ).astype(jnp.float32)
    mixed32 = (residual.astype(jnp.float32) + projected).astype(jnp.bfloat16).astype(jnp.float32)
    scale = lax.rsqrt(jnp.mean(mixed32 * mixed32, axis=-1, keepdims=True) + 1e-06)
    normed = (mixed32 * scale * norm_gain).astype(jnp.bfloat16)
    all_rows = lax.all_gather(normed, "tp", axis=0, tiled=True)
    before = jnp.dot(
        all_rows,
        lax.all_gather(up_weight, "sp", axis=0, tiled=True),
        preferred_element_type=jnp.float32,
    )
    hidden = jnp.square(jax.nn.relu(before)).astype(jnp.bfloat16)
    terms = jnp.dot(
        hidden,
        lax.all_gather(down_weight, "sp", axis=1, tiled=True),
        preferred_element_type=jnp.float32,
    )
    down = lax.psum_scatter(
        terms.astype(jnp.bfloat16), "tp", scatter_dimension=0, tiled=True
    ).astype(jnp.float32)
    return (mixed32 + down).astype(jnp.bfloat16)


LEAD = 3
PIECES = 2
CHUNKS = 2 * PIECES
F32 = jnp.float32
BF16 = jnp.bfloat16


def remote(src, dst, send_sem, recv_sem, device_id):
    return pltpu.make_async_remote_copy(
        src_ref=src,
        dst_ref=dst,
        send_sem=send_sem,
        recv_sem=recv_sem,
        device_id=device_id,
        device_id_type=pl.DeviceIdType.MESH,
    )


def aligned(value, size):
    return pl.multiple_of(value * size, size)


def layer_kernel(
    n,
    queries,
    keys,
    values,
    sink,
    out_weight,
    residual,
    gain,
    up,
    down,
    out,
    q_buf,
    k_buf,
    v_buf,
    k_wide,
    v_wide,
    attended,
    att_all,
    ow_buf,
    res_buf,
    mixed,
    normed,
    up_buf,
    down_buf,
    acc,
    hidden,
    terms,
    pair_in,
    chip_sum,
    peer_in,
    local_sem,
    tail_send,
    tail_recv,
    z_send,
    twin_send,
    y_send,
    w_recv,
    att_send,
    att_recv,
    norm_send,
    norm_recv,
    pair_send,
    pair_recv,
    peer_send,
    peer_recv,
):
    z = lax.axis_index("sp")
    y = lax.axis_index("grp")
    me = lax.axis_index("tp")
    partner = me + 1 - 2 * lax.rem(me, 2)
    across = lax.rem(me + 2, 4)
    diagonal = lax.rem(partner + 2, 4)
    rows, head_cols = q_buf.shape
    own = rows // 4
    depth = up.shape[0]
    width = down.shape[1]
    cols = up.shape[1]
    wide = n * width
    part = width // 2
    lane = part // 2
    chunk = (depth // 2 // CHUNKS, down.shape[0] // PIECES)
    near = jnp.minimum(z, n - 1 - z)
    is_end = near == 0
    far_sign = jnp.where(z < n - 1 - z, 1, -1)

    barrier = pltpu.get_barrier_semaphore()
    for step in range(1, 4):
        pl.semaphore_signal(
            barrier,
            inc=1,
            device_id={"tp": lax.rem(me + step, 4)},
            device_id_type=pl.DeviceIdType.MESH,
        )
    pl.semaphore_signal(
        barrier, inc=1, device_id={"grp": 1 - y}, device_id_type=pl.DeviceIdType.MESH
    )

    @pl.when(z > 0)
    def _():
        pl.semaphore_signal(
            barrier, inc=1, device_id={"sp": z - 1}, device_id_type=pl.DeviceIdType.MESH
        )

    @pl.when(z < n - 1)
    def _():
        pl.semaphore_signal(
            barrier, inc=1, device_id={"sp": z + 1}, device_id_type=pl.DeviceIdType.MESH
        )

    own_up = up_buf.at[pl.ds(aligned(z, depth), depth), :]
    locals_ = [
        pltpu.make_async_copy(keys, k_buf.at[:, pl.ds(WINDOW, rows)], local_sem.at[0]),
        pltpu.make_async_copy(values, v_buf.at[:, pl.ds(WINDOW, rows)], local_sem.at[1]),
        pltpu.make_async_copy(queries, q_buf, local_sem.at[2]),
        pltpu.make_async_copy(out_weight, ow_buf, local_sem.at[3]),
        pltpu.make_async_copy(residual, res_buf, local_sem.at[4]),
        pltpu.make_async_copy(up, own_up, local_sem.at[5]),
    ]
    for index in range(4):
        source = down.at[:, pl.ds(index * lane, lane)]
        place = down_buf.at[z, index // 2, index % 2]
        locals_.append(pltpu.make_async_copy(source, place, local_sem.at[6 + index]))
    for copy in locals_:
        copy.start()

    edge = jnp.where(z > 0, 1, 0) + jnp.where(z < n - 1, 1, 0)
    pl.semaphore_wait(barrier, 4 + edge)

    def piece(weight, owner, half, index):
        if weight == 0:
            start = owner * depth + half * (depth // 2) + index * chunk[0]
            return up_buf.at[pl.ds(pl.multiple_of(start, chunk[0]), chunk[0]), :]
        return down_buf.at[
            owner, index // PIECES, half, pl.ds(aligned(index % PIECES, chunk[1]), chunk[1]), :
        ]

    def own_piece(weight, half, index):
        if weight == 0:
            start = half * (depth // 2) + index * chunk[0]
            return up.at[pl.ds(pl.multiple_of(start, chunk[0]), chunk[0]), :]
        return piece(weight, z, half, index)

    def z_copy(weight, owner, index, upward, source=None):
        place = piece(weight, owner, y, index)
        return remote(
            place if source is None else source,
            place,
            z_send.at[upward, weight, owner, index],
            w_recv.at[weight, owner, y, index],
            {"sp": z + (1 if upward else -1)},
        )

    def twin_copy(weight, index):
        return remote(
            own_piece(weight, 1 - y, index),
            piece(weight, z, 1 - y, index),
            twin_send.at[weight, index],
            w_recv.at[weight, z, 1 - y, index],
            {"sp": z + far_sign},
        )

    def y_copy(weight, owner, index):
        place = piece(weight, owner, y, index)
        return remote(
            place,
            place,
            y_send.at[weight, owner, index],
            w_recv.at[weight, owner, y, index],
            {"grp": 1 - y},
        )

    def has_twin(owner):
        return ((z == 1) & (owner == 0)) | ((z == n - 2) & (owner == n - 1))

    def wait_piece(weight, owner, half, index):
        place = piece(weight, owner, half, index)
        remote(
            place,
            place,
            y_send.at[weight, owner, index],
            w_recv.at[weight, owner, half, index],
            {"grp": 1 - y},
        ).wait_recv()

    def each_piece(action):
        def step(index, carry):
            action(index)
            return carry

        lax.fori_loop(0, CHUNKS, step, 0)

    def send_own(weight, upward):
        each_piece(lambda index: z_copy(weight, z, index, upward, own_piece(weight, y, index)).start())

    def tail_copy(which):
        source, place = ((keys, k_buf), (values, v_buf))[which]
        return remote(
            source.at[:, pl.ds(rows - WINDOW, WINDOW)],
            place.at[:, pl.ds(0, WINDOW)],
            tail_send.at[which],
            tail_recv.at[which],
            {"sp": z + 1},
        )

    @pl.when(z < n - 1)
    def _():
        tail_copy(0).start()
        tail_copy(1).start()
        send_own(0, 1)

    @pl.when(z > 0)
    def _():
        send_own(0, 0)

    @pl.when(is_end)
    def _():
        each_piece(lambda index: twin_copy(0, index).start())

    def owner_at(order):
        close = order <= 2 * near
        side = 2 * lax.rem(order + 1, 2) - 1
        return z + jnp.where(close, side * ((order + 1) // 2), far_sign * (order - near))

    def unit_at(unit):
        close = unit < near * 4
        rest = jnp.maximum(unit - near * 4, 0)
        side = 2 * (unit % 2) - 1
        owner = z + jnp.where(
            close, side * (unit // 4 + 1), far_sign * (near + 1 + lax.div(rest, 2))
        )
        return owner, jnp.where(close, (unit % 4) // 2, lax.rem(rest, 2))

    def shard_at(number):
        owner, block = unit_at(number // PIECES)
        return owner, block * PIECES + number % PIECES

    def event(weight, number):
        owner, index = shard_at(number)
        wait_piece(weight, owner, y, index)

        @pl.when((owner < z) & (z < n - 1))
        def _():
            z_copy(weight, owner, index, 1).start()

        @pl.when((owner > z) & (z > 0))
        def _():
            z_copy(weight, owner, index, 0).start()

        @pl.when(jnp.logical_not(has_twin(owner)))
        def _():
            y_copy(weight, owner, index).start()

    total = (n - 1) * CHUNKS

    def pick(end, middle):
        return end if end == middle else jnp.where(is_end, end, middle)

    def run(action, weight, state, goals):
        starts = [min(max(at - weight * total, 0), total) for at in state]
        stops = [min(max(at - weight * total, 0), total) for at in goals]
        if starts == stops:
            return

        def step(number, carry):
            action(weight, number)
            return carry

        lax.fori_loop(pick(*starts), pick(*stops), step, 0)

    arrived = [0, 0]
    halves = [0, 0]

    def scaled(count):
        return min(count * CHUNKS // 4, 2 * total)

    def advance(end, middle):
        goals = [max(arrived[0], scaled(end)), max(arrived[1], scaled(middle))]
        run(event, 0, arrived, goals)
        if arrived[1] < total <= goals[1]:

            @pl.when(jnp.logical_not(is_end))
            def _():
                send_own(1, 1)
                send_own(1, 0)

        run(event, 1, arrived, goals)
        arrived[:] = goals

    def take_half(weight, number):
        owner, index = shard_at(number)
        wait_piece(weight, owner, 1 - y, index)

    def take(end, middle):
        goals = [max(halves[0], scaled(end)), max(halves[1], scaled(middle))]
        assert goals[0] <= arrived[0] and goals[1] <= arrived[1]
        run(take_half, 0, halves, goals)
        run(take_half, 1, halves, goals)
        halves[:] = goals

    @pl.when(z == 0)
    def _():
        k_buf[:, pl.ds(0, WINDOW)] = jnp.zeros((HEAD_DIM, WINDOW), BF16)
        v_buf[:, pl.ds(0, WINDOW)] = jnp.zeros((HEAD_DIM, WINDOW), BF16)

    for copy in (*locals_[:3], *locals_[6:]):
        copy.wait()

    @pl.when(is_end)
    def _():
        @pl.when(z < n - 1)
        def _():
            send_own(1, 1)

        @pl.when(z > 0)
        def _():
            send_own(1, 0)

        each_piece(lambda index: twin_copy(1, index).start())

    @pl.when(z > 0)
    def _():
        tail_copy(0).wait_recv()
        tail_copy(1).wait_recv()

    heads = head_cols // HEAD_DIM
    for h in range(heads):
        k_wide[h * HEAD_DIM : (h + 1) * HEAD_DIM, :] = k_buf[...]
        v_wide[h * HEAD_DIM : (h + 1) * HEAD_DIM, :] = v_buf[...]

    def attend(block, carry):
        start = aligned(block, WINDOW)
        q_rows = q_buf[pl.ds(start, WINDOW), :].astype(F32)
        lane_head = lax.broadcasted_iota(jnp.int32, (WINDOW, head_cols), 1) // HEAD_DIM
        stacked = jnp.concatenate(
            [jnp.where(lane_head == h, q_rows, 0.0) for h in range(heads)], axis=0
        ).astype(BF16)
        scores = jnp.dot(
            stacked, k_wide[:, pl.ds(start, 2 * WINDOW)], preferred_element_type=F32
        ) * HEAD_DIM ** (-0.5)
        i = lax.broadcasted_iota(jnp.int32, (heads * WINDOW, 2 * WINDOW), 0) % WINDOW
        j = lax.broadcasted_iota(jnp.int32, (heads * WINDOW, 2 * WINDOW), 1)
        first = WINDOW - z * rows - block * WINDOW
        valid = (j > i) & (j <= i + WINDOW) & (j >= first)
        scores = jnp.where(valid, scores, -1e30)
        sinks = jnp.concatenate(
            [jnp.full((WINDOW, 1), sink[h], F32) for h in range(heads)], axis=0
        )
        top = jnp.maximum(jnp.max(scores, axis=-1, keepdims=True), sinks)
        weights = jnp.exp(scores - top)
        total = jnp.sum(weights, axis=-1, keepdims=True) + jnp.exp(sinks - top)
        probs = (weights / total).astype(BF16)
        mixed_heads = lax.dot_general(
            probs,
            v_wide[:, pl.ds(start, 2 * WINDOW)],
            (((1,), (1,)), ((), ())),
            preferred_element_type=F32,
        )
        result = jnp.zeros((WINDOW, head_cols), F32)
        for h in range(heads):
            result += jnp.where(
                lane_head == h, mixed_heads[h * WINDOW : (h + 1) * WINDOW], 0.0
            )
        attended[pl.ds(start, WINDOW), :] = result.astype(BF16)
        return carry

    blocks = rows // WINDOW
    for block in range(0, blocks, 2):
        lax.fori_loop(block, min(block + 2, blocks), attend, 0)
        advance((0, 1, 3)[min(block // 2, 2)], (0, 4, 6)[min(block // 2, 2)])

    def att_copy(step):
        peer = lax.rem(me + step, 4)
        return remote(
            attended.at[pl.ds(aligned(peer, own), own), :],
            att_all.at[me],
            att_send.at[step - 1],
            att_recv.at[me],
            {"tp": peer},
        )

    def att_wait(step):
        peer = lax.rem(me + step, 4)
        remote(
            att_all.at[peer], att_all.at[peer], att_send.at[step - 1], att_recv.at[peer], {"tp": peer}
        ).wait_recv()

    for step in (2, 1, 3):
        att_copy(step).start()
    att_all[me] = attended[pl.ds(aligned(me, own), own), :]
    advance(4, 8)
    locals_[3].wait()
    locals_[4].wait()
    for step in (1, 2, 3):
        att_wait(step)
    advance(5, 9)

    tile = 256

    def project(index, squares):
        span = pl.ds(aligned(index, tile), tile)
        value = res_buf[:, span].astype(F32)
        for peer in range(4):
            value += jnp.dot(
                att_all[peer],
                ow_buf[peer * head_cols : (peer + 1) * head_cols, span],
                preferred_element_type=F32,
            )
        value = value.astype(BF16).astype(F32)
        mixed[:, span] = value
        return squares + jnp.sum(value * value, axis=-1, keepdims=True)

    squares = lax.fori_loop(0, wide // tile, project, jnp.zeros((own, 1), F32))
    scale = lax.rsqrt(squares / wide + 1e-06)
    own_rows = pl.ds(aligned(me, own), own)

    def norm_copy(slot, order, source, target):
        place = normed.at[
            pl.ds(aligned(source, own), own), pl.ds(aligned(owner_at(order), depth), depth)
        ]
        return remote(
            place, place, norm_send.at[order, slot], norm_recv.at[order, source], {"tp": target}
        )

    for order in range(n):
        span = pl.ds(aligned(owner_at(order), depth), depth)
        normed[own_rows, span] = (mixed[:, span] * scale * gain[:, span]).astype(BF16)
        norm_copy(0, order, me, across).start()
        norm_copy(1, order, me, partner).start()

    locals_[5].wait()
    plan = ((7, 11), (10, 13), (11, 16), (13, 19))
    for order in range(n):
        owner = owner_at(order)
        advance(*plan[order])
        norm_copy(2, order, across, across).wait_recv()
        norm_copy(2, order, across, partner).start()
        if order != 1:
            advance(*(count + 1 for count in plan[order]))
        take(4 * order, 4 * min(order + order % 2, n - 1))
        norm_copy(2, order, partner, partner).wait_recv()
        norm_copy(2, order, diagonal, partner).wait_recv()

        def up_step(index, carry, owner=owner, order=order):
            span = pl.ds(aligned(index, tile), tile)
            value = jnp.dot(
                normed[:, pl.ds(aligned(owner, depth), depth)],
                up_buf[pl.ds(aligned(owner, depth), depth), span],
                preferred_element_type=F32,
            )
            if order:
                value += acc[:, span]
            if order == n - 1:
                hidden[:, span] = jnp.square(jnp.maximum(value, 0.0)).astype(BF16)
            else:
                acc[:, span] = value
            return carry

        lax.fori_loop(0, cols // tile, up_step, 0)

    blocks = 2 * n
    last = blocks - 1

    def place_of(which):
        if which < 2:
            return z, which, 0, part
        owner, block = unit_at(min(which, last) - 2)
        if which < last:
            return owner, block, 0, part
        return owner, block, (y if which == last else 1 - y) * lane, lane

    def pair_copy(which, slot):
        size = place_of(which)[3]
        group = (partner, diagonal)[slot]
        return remote(
            terms.at[which, pl.ds(aligned(group, own), own), pl.ds(0, size)],
            pair_in.at[which, slot, :, pl.ds(0, size)],
            pair_send.at[which, slot],
            pair_recv.at[which, slot],
            {"tp": partner},
        )

    def peer_copy(which):
        size = place_of(which)[3]
        return remote(
            chip_sum.at[which, :, pl.ds(0, size)],
            peer_in.at[which, :, pl.ds(0, size)],
            peer_send.at[which],
            peer_recv.at[which],
            {"tp": across},
        )

    def multiply(which):
        owner, block, offset, size = place_of(which)
        if size == part:
            weight = jnp.concatenate([down_buf[owner, block, half] for half in range(2)], axis=1)
        else:
            weight = down_buf[owner, block, y if which == last else 1 - y]
        terms[which, :, 0:size] = jnp.dot(
            hidden[...], weight, preferred_element_type=F32
        ).astype(BF16)
        pair_copy(which, 1).start()
        pair_copy(which, 0).start()

    def combine(which):
        size = place_of(which)[3]
        pair_copy(which, 1).wait_recv()
        other = pl.ds(aligned(across, own), own)
        chip_sum[which, :, 0:size] = (
            terms[which, other, 0:size].astype(F32) + pair_in[which, 1, :, 0:size].astype(F32)
        ).astype(BF16)
        peer_copy(which).start()

    def finish(which):
        owner, block, offset, size = place_of(which)
        target = pl.ds(pl.multiple_of(owner * width + block * part + offset, size), size)
        peer_copy(which).wait_recv()
        pair_copy(which, 0).wait_recv()
        value = (
            terms[which, own_rows, 0:size].astype(F32)
            + pair_in[which, 0, :, 0:size].astype(F32)
            + peer_in[which, :, 0:size].astype(F32)
        )
        out[:, target] = (mixed[:, target] + value).astype(BF16)

    first = 4 * (n - 1)
    for which in range(blocks + 1):
        ready = first + 2 * (min(which, last) - 1)
        if which < 2:
            advance(first + 3 + which, first + 7 + which)
        elif which != last:
            for step in range(2):
                advance(ready - 1 + step + LEAD, ready + 6)
                take(ready - 1 + step, ready - 1 + step)
        else:
            advance(ready, ready + 6)
        multiply(which)
        combine(which)
        if which == 1:
            advance(first + 5, first + 9)
        if which:
            finish(which - 1)
    finish(blocks)

    for step in (1, 2, 3):
        att_copy(step).wait_send()
    for order in range(n):
        norm_copy(0, order, me, across).wait_send()
        norm_copy(1, order, me, partner).wait_send()
        norm_copy(2, order, across, partner).wait_send()
    for which in range(blocks + 1):
        pair_copy(which, 0).wait_send()
        pair_copy(which, 1).wait_send()
        peer_copy(which).wait_send()

    @pl.when(z < n - 1)
    def _():
        tail_copy(0).wait_send()
        tail_copy(1).wait_send()

    for weight in range(2):

        @pl.when(is_end)
        def _():
            each_piece(lambda index: twin_copy(weight, index).wait_send())

        for owner in range(n):

            @pl.when((z >= owner) & (z < n - 1))
            def _():
                each_piece(lambda index: z_copy(weight, owner, index, 1).wait_send())

            @pl.when((z <= owner) & (z > 0))
            def _():
                each_piece(lambda index: z_copy(weight, owner, index, 0).wait_send())

            @pl.when((z != owner) & jnp.logical_not(has_twin(owner)))
            def _():
                each_piece(lambda index: y_copy(weight, owner, index).wait_send())


def fused_body(
    n,
    queries,
    key_rows,
    value_rows,
    sink_logits,
    out_weight,
    residual,
    norm_gain,
    up_weight,
    down_weight,
):
    rows, head_cols = queries.shape
    own, wide = residual.shape
    depth, cols = up_weight.shape
    width = down_weight.shape[1]
    part = width // 2
    vmem = lambda *shape: pltpu.VMEM(shape, BF16)
    dma = lambda *shape: pltpu.SemaphoreType.DMA(shape)
    hbm = pl.BlockSpec(memory_space=pl.ANY)
    return pl.pallas_call(
        functools.partial(layer_kernel, n),
        out_shape=pltpu.VMEM((own, wide), BF16),
        in_specs=[
            hbm,
            hbm,
            hbm,
            pl.BlockSpec(memory_space=pltpu.SMEM),
            hbm,
            hbm,
            pl.BlockSpec(memory_space=pltpu.VMEM),
            hbm,
            hbm,
        ],
        out_specs=pl.BlockSpec(memory_space=pltpu.VMEM),
        scratch_shapes=[
            vmem(rows, head_cols),
            vmem(HEAD_DIM, rows + WINDOW),
            vmem(HEAD_DIM, rows + WINDOW),
            vmem(head_cols, rows + WINDOW),
            vmem(head_cols, rows + WINDOW),
            vmem(rows, head_cols),
            vmem(4, own, head_cols),
            vmem(*out_weight.shape),
            vmem(own, wide),
            pltpu.VMEM((own, wide), F32),
            vmem(rows, wide),
            vmem(n * depth, cols),
            vmem(n, 2, 2, cols, part // 2),
            pltpu.VMEM((rows, cols), F32),
            vmem(rows, cols),
            vmem(2 * n + 1, rows, part),
            vmem(2 * n + 1, 2, own, part),
            vmem(2 * n + 1, own, part),
            vmem(2 * n + 1, own, part),
            dma(10),
            dma(2),
            dma(2),
            dma(2, 2, n, CHUNKS),
            dma(2, CHUNKS),
            dma(2, n, CHUNKS),
            dma(2, n, 2, CHUNKS),
            dma(3),
            dma(4),
            dma(n, 3),
            dma(n, 4),
            dma(2 * n + 1, 2),
            dma(2 * n + 1, 2),
            dma(2 * n + 1),
            dma(2 * n + 1),
        ],
        compiler_params=pltpu.CompilerParams(
            collective_id=0, has_side_effects=True, vmem_limit_bytes=60 * 1024 * 1024
        ),
    )(
        queries,
        key_rows.T,
        value_rows.T,
        sink_logits,
        out_weight,
        residual,
        norm_gain.reshape(1, -1),
        up_weight,
        down_weight,
    )


def solution(mesh):
    in_specs = (
        P(("grp", "sp"), "tp"),
        P(("grp", "sp"), "tp"),
        P(("grp", "sp"), "tp"),
        P("tp"),
        P(),
        P(("grp", "sp", "tp"), None),
        P(),
        P("sp", "tp"),
        P("tp", "sp"),
    )
    out_specs = P(("grp", "sp", "tp"), None)
    n = mesh.shape["sp"]

    def layer(*arrays):
        key_rows, up_weight, down_weight = arrays[1], arrays[7], arrays[8]
        fits = (
            n == 4
            and mesh.shape["grp"] == 2
            and mesh.shape["tp"] == 4
            and key_rows.shape[1] == HEAD_DIM
            and up_weight.shape[0] % (32 * CHUNKS) == 0
            and up_weight.shape[1] % 256 == 0
            and down_weight.shape[1] % 512 == 0
        )
        return (functools.partial(fused_body, n) if fits else body)(*arrays)

    return jax.shard_map(layer, mesh=mesh, in_specs=in_specs, out_specs=out_specs, check_vma=False)
```

```python
import functools

import jax
import jax.numpy as jnp
from jax import lax
from jax.experimental import pallas as pl
from jax.experimental.pallas import tpu as pltpu
from jax.sharding import PartitionSpec as P

HEAD_DIM = 64
WINDOW = 128


def shifted(value, axis, steps):
    count = lax.axis_size(axis)
    leading, last = (max(0, -steps), min(count, count - steps))
    return lax.ppermute(value, axis, [(source, source + steps) for source in range(leading, last)])


def band_attend(queries, key_rows, value_rows, sink_logits, tail_keys, tail_values, offset):
    rows = queries.shape[0]
    kv_heads = key_rows.shape[1] // HEAD_DIM
    group = queries.shape[1] // (kv_heads * HEAD_DIM)
    blocks = rows // WINDOW
    all_keys = jnp.concatenate([tail_keys, key_rows], axis=0).reshape(
        blocks + 1, WINDOW, kv_heads, HEAD_DIM
    )
    all_values = jnp.concatenate([tail_values, value_rows], axis=0).reshape(
        blocks + 1, WINDOW, kv_heads, HEAD_DIM
    )
    key_blocks = jnp.concatenate([all_keys[:-1], all_keys[1:]], axis=1)
    value_blocks = jnp.concatenate([all_values[:-1], all_values[1:]], axis=1)
    query_blocks = queries.reshape(blocks, WINDOW, kv_heads, group, HEAD_DIM)
    scores = jnp.einsum(
        "nqkgd,nskd->nkgqs", query_blocks, key_blocks, preferred_element_type=jnp.float32
    ) * HEAD_DIM ** (-0.5)
    q_local = jnp.arange(WINDOW, dtype=jnp.int32) + WINDOW
    k_local = jnp.arange(2 * WINDOW, dtype=jnp.int32)
    distance = q_local[:, None] - k_local[None, :]
    key_position = (
        offset + (jnp.arange(blocks, dtype=jnp.int32)[:, None] - 1) * WINDOW + k_local[None, :]
    )
    valid = ((distance >= 0) & (distance < WINDOW))[None] & (key_position >= 0)[:, None, :]
    scores = jnp.where(valid[:, None, None], scores, -1e30)
    sink = sink_logits.reshape(kv_heads, group)[None, :, :, None, None]
    top = jnp.maximum(jnp.max(scores, axis=-1, keepdims=True), sink)
    weights = jnp.exp(scores - top)
    total = jnp.sum(weights, axis=-1, keepdims=True) + jnp.exp(sink - top)
    probs = (weights / total).astype(jnp.bfloat16)
    result = jnp.einsum(
        "nkgqs,nskd->nqkgd", probs, value_blocks, preferred_element_type=jnp.float32
    )
    return result.astype(jnp.bfloat16).reshape(rows, kv_heads * group * HEAD_DIM)


def body(
    queries,
    key_rows,
    value_rows,
    sink_logits,
    out_weight,
    residual,
    norm_gain,
    up_weight,
    down_weight,
):
    rows = queries.shape[0]
    width = key_rows.shape[1]
    kv_pair = jnp.concatenate([key_rows[rows - WINDOW :], value_rows[rows - WINDOW :]], axis=1)
    tail = shifted(kv_pair, "sp", 1)
    offset = lax.axis_index("sp") * rows
    attended = band_attend(
        queries, key_rows, value_rows, sink_logits, tail[:, :width], tail[:, width:], offset
    )
    head_cols = attended.shape[1]
    own_rows = lax.dynamic_slice_in_dim(out_weight, lax.axis_index("tp") * head_cols, head_cols, 0)
    projected = lax.psum_scatter(
        jnp.dot(attended, own_rows, preferred_element_type=jnp.float32).astype(jnp.bfloat16),
        "tp",
        scatter_dimension=0,
        tiled=True,
    ).astype(jnp.float32)
    mixed32 = (residual.astype(jnp.float32) + projected).astype(jnp.bfloat16).astype(jnp.float32)
    scale = lax.rsqrt(jnp.mean(mixed32 * mixed32, axis=-1, keepdims=True) + 1e-06)
    normed = (mixed32 * scale * norm_gain).astype(jnp.bfloat16)
    all_rows = lax.all_gather(normed, "tp", axis=0, tiled=True)
    before = jnp.dot(
        all_rows,
        lax.all_gather(up_weight, "sp", axis=0, tiled=True),
        preferred_element_type=jnp.float32,
    )
    hidden = jnp.square(jax.nn.relu(before)).astype(jnp.bfloat16)
    terms = jnp.dot(
        hidden,
        lax.all_gather(down_weight, "sp", axis=1, tiled=True),
        preferred_element_type=jnp.float32,
    )
    down = lax.psum_scatter(
        terms.astype(jnp.bfloat16), "tp", scatter_dimension=0, tiled=True
    ).astype(jnp.float32)
    return (mixed32 + down).astype(jnp.bfloat16)


PIECES = 4
HOP = 4.7
PACE = 2.8
CHUNKS = 2 * PIECES
F32 = jnp.float32
BF16 = jnp.bfloat16


def remote(src, dst, send_sem, recv_sem, device_id):
    return pltpu.make_async_remote_copy(
        src_ref=src,
        dst_ref=dst,
        send_sem=send_sem,
        recv_sem=recv_sem,
        device_id=device_id,
        device_id_type=pl.DeviceIdType.MESH,
    )


def aligned(value, size):
    return pl.multiple_of(value * size, size)


def layer_kernel(
    n,
    queries,
    keys,
    values,
    sink_in,
    out_weight,
    residual,
    gain_in,
    up,
    down,
    out,
    sink,
    gain,
    out_buf,
    q_buf,
    kv_buf,
    k_wide,
    v_wide,
    attended,
    att_all,
    ow_buf,
    res_buf,
    mixed,
    normed,
    up_buf,
    down_buf,
    acc,
    hidden,
    terms,
    pair_in,
    chip_sum,
    peer_in,
    local_sem,
    tail_sem,
    z_send,
    twin_send,
    y_send,
    z_recv,
    y_up,
    y_down,
    att_sem,
    norm_send,
    norm_recv,
    send_sem,
    pair_recv,
    peer_recv,
):
    z = lax.axis_index("sp")
    y = lax.axis_index("grp")
    me = lax.axis_index("tp")
    partner = me + 1 - 2 * lax.rem(me, 2)
    across = lax.rem(me + 2, 4)
    diagonal = lax.rem(partner + 2, 4)
    rows, head_cols = q_buf.shape
    own = rows // 4
    depth = up.shape[0]
    width = down.shape[1]
    cols = up.shape[1]
    wide = n * width
    part = width // 2
    lane = part // 2
    chunk = (depth // 2 // CHUNKS, down.shape[0] // PIECES)
    near = jnp.minimum(z, n - 1 - z)
    is_end = near == 0
    far_sign = jnp.where(z < n - 1 - z, 1, -1)

    barrier = pltpu.get_barrier_semaphore()
    for step in range(1, 4):
        pl.semaphore_signal(
            barrier,
            inc=1,
            device_id={"tp": lax.rem(me + step, 4)},
            device_id_type=pl.DeviceIdType.MESH,
        )
    pl.semaphore_signal(
        barrier, inc=1, device_id={"grp": 1 - y}, device_id_type=pl.DeviceIdType.MESH
    )

    @pl.when(z > 0)
    def _():
        pl.semaphore_signal(
            barrier, inc=1, device_id={"sp": z - 1}, device_id_type=pl.DeviceIdType.MESH
        )

    @pl.when(z < n - 1)
    def _():
        pl.semaphore_signal(
            barrier, inc=1, device_id={"sp": z + 1}, device_id_type=pl.DeviceIdType.MESH
        )

    own_up = up_buf.at[pl.ds(aligned(z, depth), depth), :]
    wait_of = lambda ref, sem: pltpu.make_async_copy(ref, ref, sem).wait()
    pltpu.make_async_copy(keys, kv_buf.at[0, :, pl.ds(WINDOW, rows)], local_sem.at[0]).start()
    pltpu.make_async_copy(values, kv_buf.at[1, :, pl.ds(WINDOW, rows)], local_sem.at[0]).start()
    for index in range(4):
        source = down.at[:, pl.ds(index * lane, lane)]
        place = down_buf.at[z, index // 2, index % 2]
        pltpu.make_async_copy(source, place, local_sem.at[1]).start()
    locals_ = [
        pltpu.make_async_copy(queries, q_buf, local_sem.at[2]),
        pltpu.make_async_copy(sink_in, sink, local_sem.at[3]),
        pltpu.make_async_copy(out_weight, ow_buf, local_sem.at[4]),
        pltpu.make_async_copy(residual, res_buf, local_sem.at[5]),
        pltpu.make_async_copy(gain_in, gain, local_sem.at[6]),
        pltpu.make_async_copy(up, own_up, local_sem.at[7]),
    ]
    for copy in locals_:
        copy.start()

    edge = jnp.where(z > 0, 1, 0) + jnp.where(z < n - 1, 1, 0)
    pl.semaphore_wait(barrier, 4 + edge)

    def piece(weight, owner, half, index):
        if weight == 0:
            start = owner * depth + half * (depth // 2) + index * chunk[0]
            return up_buf.at[pl.ds(pl.multiple_of(start, chunk[0]), chunk[0]), :]
        return down_buf.at[
            owner, index // PIECES, half, pl.ds(aligned(index % PIECES, chunk[1]), chunk[1]), :
        ]

    def own_piece(weight, half, index):
        if weight == 0:
            start = half * (depth // 2) + index * chunk[0]
            return up.at[pl.ds(pl.multiple_of(start, chunk[0]), chunk[0]), :]
        return piece(weight, z, half, index)

    def half_of(weight, owner, half):
        if weight == 0:
            start = owner * depth + half * (depth // 2)
            return up_buf.at[pl.ds(pl.multiple_of(start, depth // 2), depth // 2), :]
        return down_buf.at[owner, :, half]

    def slot_of(owner, position):
        return lax.rem(owner - position + n, n) - 1

    def z_slot(owner, upward):
        return owner if upward else jnp.where(owner == z, n, owner)

    def z_copy(weight, owner, index, upward, source=None):
        place = piece(weight, owner, y, index)
        target = z + (1 if upward else -1)
        return remote(
            place if source is None else source,
            place,
            z_send.at[weight, z_slot(owner, upward)],
            z_recv.at[weight, slot_of(owner, target), index],
            {"sp": target},
        )

    def half_sem(weight, owner, position, index):
        if weight == 0:
            return y_up.at[slot_of(owner, position)]
        return y_down.at[slot_of(owner, position), index // (PIECES // 2)]

    def twin_copy(weight, index):
        return remote(
            own_piece(weight, 1 - y, index),
            piece(weight, z, 1 - y, index),
            twin_send.at[weight],
            half_sem(weight, z, z + far_sign, index),
            {"sp": z + far_sign},
        )

    def y_copy(weight, owner, index):
        place = piece(weight, owner, y, index)
        return remote(
            place,
            place,
            y_send.at[weight, slot_of(owner, z)],
            half_sem(weight, owner, z, index),
            {"grp": 1 - y},
        )

    def has_twin(owner):
        return ((z == 1) & (owner == 0)) | ((z == n - 2) & (owner == n - 1))

    def each_piece(action):
        def step(index, carry):
            action(index)
            return carry

        lax.fori_loop(0, CHUNKS, step, 0)

    def send_own(weight, upward):
        each_piece(lambda index: z_copy(weight, z, index, upward, own_piece(weight, y, index)).start())

    def tail_copy(which):
        return remote(
            (keys, values)[which].at[:, pl.ds(rows - WINDOW, WINDOW)],
            kv_buf.at[which, :, pl.ds(0, WINDOW)],
            tail_sem.at[0],
            tail_sem.at[1],
            {"sp": z + 1},
        )

    @pl.when(z < n - 1)
    def _():
        tail_copy(0).start()
        tail_copy(1).start()
        send_own(0, 1)

    @pl.when(z > 0)
    def _():
        send_own(0, 0)

    @pl.when(is_end)
    def _():
        each_piece(lambda index: twin_copy(0, index).start())

    def owner_at(order):
        close = order <= 2 * near
        side = 2 * lax.rem(order + 1, 2) - 1
        return z + jnp.where(close, side * ((order + 1) // 2), far_sign * (order - near))

    def unit_at(unit):
        close = unit < near * 4
        rest = jnp.maximum(unit - near * 4, 0)
        side = 2 * (unit % 2) - 1
        owner = z + jnp.where(
            close, side * (unit // 4 + 1), far_sign * (near + 1 + lax.div(rest, 2))
        )
        return owner, jnp.where(close, (unit % 4) // 2, lax.rem(rest, 2))

    def shard_at(number):
        owner, block = unit_at(number // PIECES)
        return owner, block * PIECES + number % PIECES

    def event(weight, number):
        owner, index = shard_at(number)
        wait_of(piece(weight, owner, y, index), z_recv.at[weight, slot_of(owner, z), index])

        @pl.when((owner < z) & (z < n - 1))
        def _():
            z_copy(weight, owner, index, 1).start()

        @pl.when((owner > z) & (z > 0))
        def _():
            z_copy(weight, owner, index, 0).start()

        @pl.when(jnp.logical_not(has_twin(owner)))
        def _():
            y_copy(weight, owner, index).start()

    total = (n - 1) * CHUNKS

    def pick(end, middle):
        return end if end == middle else jnp.where(is_end, end, middle)

    arrived = [0, 0]

    def run(weight, goals):
        starts = [min(max(at - weight * total, 0), total) for at in arrived]
        stops = [min(max(at - weight * total, 0), total) for at in goals]
        if starts == stops:
            return

        def step(number, carry):
            event(weight, number)
            return carry

        lax.fori_loop(pick(*starts), pick(*stops), step, 0)

    def advance(end, middle):
        goals = [max(arrived[0], min(end, 2 * total)), max(arrived[1], min(middle, 2 * total))]
        run(0, goals)
        if arrived[1] < total <= goals[1]:

            @pl.when(jnp.logical_not(is_end))
            def _():
                send_own(1, 1)
                send_own(1, 0)

        run(1, goals)
        arrived[:] = goals

    def forward(clock):
        fine = PACE * 4 / CHUNKS
        landed = lambda since: max(int((clock - HOP - since) // fine), 0)
        middle = 0
        for since in (0, 8 * PACE):
            side = min(landed(since), CHUNKS)
            middle += 2 * PIECES * (side // PIECES) + side % PIECES
            middle += min(max(landed(since) - CHUNKS, 0), CHUNKS)
        advance(landed(0), middle)

    @pl.when(z == 0)
    def _():
        kv_buf[:, :, pl.ds(0, WINDOW)] = jnp.zeros((2, HEAD_DIM, WINDOW), BF16)

    wait_of(kv_buf.at[:, :, pl.ds(WINDOW, rows)], local_sem.at[0])
    wait_of(down_buf.at[z], local_sem.at[1])
    for copy in locals_[:2]:
        copy.wait()

    @pl.when(is_end)
    def _():
        @pl.when(z < n - 1)
        def _():
            send_own(1, 1)

        @pl.when(z > 0)
        def _():
            send_own(1, 0)

        each_piece(lambda index: twin_copy(1, index).start())

    @pl.when(z > 0)
    def _():
        wait_of(kv_buf.at[:, :, pl.ds(0, WINDOW)], tail_sem.at[1])

    heads = head_cols // HEAD_DIM
    for h in range(heads):
        k_wide[h * HEAD_DIM : (h + 1) * HEAD_DIM, :] = kv_buf[0]
        v_wide[h * HEAD_DIM : (h + 1) * HEAD_DIM, :] = kv_buf[1]

    def attend(block, carry):
        start = aligned(block, WINDOW)
        q_rows = q_buf[pl.ds(start, WINDOW), :].astype(F32)
        lane_head = lax.broadcasted_iota(jnp.int32, (WINDOW, head_cols), 1) // HEAD_DIM
        stacked = jnp.concatenate(
            [jnp.where(lane_head == h, q_rows, 0.0) for h in range(heads)], axis=0
        ).astype(BF16)
        scores = jnp.dot(
            stacked, k_wide[:, pl.ds(start, 2 * WINDOW)], preferred_element_type=F32
        ) * HEAD_DIM ** (-0.5)
        i = lax.broadcasted_iota(jnp.int32, (heads * WINDOW, 2 * WINDOW), 0) % WINDOW
        j = lax.broadcasted_iota(jnp.int32, (heads * WINDOW, 2 * WINDOW), 1)
        first = WINDOW - z * rows - block * WINDOW
        valid = (j > i) & (j <= i + WINDOW) & (j >= first)
        scores = jnp.where(valid, scores, -1e30)
        sinks = jnp.concatenate(
            [jnp.full((WINDOW, 1), sink[h], F32) for h in range(heads)], axis=0
        )
        top = jnp.maximum(jnp.max(scores, axis=-1, keepdims=True), sinks)
        weights = jnp.exp(scores - top)
        total = jnp.sum(weights, axis=-1, keepdims=True) + jnp.exp(sinks - top)
        probs = (weights / total).astype(BF16)
        mixed_heads = lax.dot_general(
            probs,
            v_wide[:, pl.ds(start, 2 * WINDOW)],
            (((1,), (1,)), ((), ())),
            preferred_element_type=F32,
        )
        result = jnp.zeros((WINDOW, head_cols), F32)
        for h in range(heads):
            result += jnp.where(
                lane_head == h, mixed_heads[h * WINDOW : (h + 1) * WINDOW], 0.0
            )
        attended[pl.ds(start, WINDOW), :] = result.astype(BF16)
        return carry

    blocks = rows // WINDOW
    for block in range(blocks):
        lax.fori_loop(block, block + 1, attend, 0)
        forward(5.5 + 1.35 * block)

    def att_copy(step):
        peer = lax.rem(me + step, 4)
        return remote(
            attended.at[pl.ds(aligned(peer, own), own), :],
            att_all.at[me],
            att_sem.at[0],
            att_sem.at[1],
            {"tp": peer},
        )

    for step in (2, 1, 3):
        att_copy(step).start()
    att_all[me] = attended[pl.ds(aligned(me, own), own), :]
    forward(14.5)
    for copy in locals_[2:5]:
        copy.wait()
    forward(16)
    wait_of(att_all.at[pl.ds(0, 3)], att_sem.at[1])
    forward(18)

    tile = 256

    def project(index, squares):
        span = pl.ds(aligned(index, tile), tile)
        value = res_buf[:, span].astype(F32)
        for peer in range(4):
            value += jnp.dot(
                att_all[peer],
                ow_buf[peer * head_cols : (peer + 1) * head_cols, span],
                preferred_element_type=F32,
            )
        value = value.astype(BF16).astype(F32)
        mixed[:, span] = value
        return squares + jnp.sum(value * value, axis=-1, keepdims=True)

    squares = lax.fori_loop(0, wide // tile // 2, project, jnp.zeros((own, 1), F32))
    forward(19.5)
    squares = lax.fori_loop(wide // tile // 2, wide // tile, project, squares)
    forward(21)
    scale = lax.rsqrt(squares / wide + 1e-06)
    own_rows = pl.ds(aligned(me, own), own)

    def norm_copy(slot, order, source, target):
        place = normed.at[
            pl.ds(aligned(source, own), own), pl.ds(aligned(owner_at(order), depth), depth)
        ]
        link = 0 if slot == 0 else 1
        return remote(place, place, norm_send.at[slot], norm_recv.at[order, link], {"tp": target})

    for order in range(n):
        span = pl.ds(aligned(owner_at(order), depth), depth)
        normed[own_rows, span] = (mixed[:, span] * scale * gain[:, span]).astype(BF16)
        norm_copy(0, order, me, across).start()
        norm_copy(1, order, me, partner).start()

    locals_[5].wait()
    clocks = (29.2, 33.2, 37.4, 41.6)
    for order in range(n):
        owner = owner_at(order)
        forward(clocks[order] - 3)
        forward(clocks[order] - 1.5)
        span = pl.ds(aligned(owner, depth), depth)
        wait_of(normed.at[own_rows, span], norm_recv.at[order, 0])
        norm_copy(2, order, across, partner).start()
        forward(clocks[order])
        if order:
            advance(order * CHUNKS, min(order + order % 2, n - 1) * CHUNKS)
            wait_of(half_of(0, owner, 1 - y), y_up.at[slot_of(owner, z)])
        wait_of(normed.at[pl.ds(0, 2 * own), span], norm_recv.at[order, 1])

        def up_step(index, carry, owner=owner, order=order):
            span = pl.ds(aligned(index, tile), tile)
            value = jnp.dot(
                normed[:, pl.ds(aligned(owner, depth), depth)],
                up_buf[pl.ds(aligned(owner, depth), depth), span],
                preferred_element_type=F32,
            )
            if order:
                value += acc[:, span]
            if order == n - 1:
                hidden[:, span] = jnp.square(jnp.maximum(value, 0.0)).astype(BF16)
            else:
                acc[:, span] = value
            return carry

        lax.fori_loop(0, cols // tile, up_step, 0)

    blocks = 2 * n
    last = blocks - 1

    def place_of(which):
        if which < 2:
            return z, which, 0, part
        owner, block = unit_at(min(which, last) - 2)
        if which < last:
            return owner, block, 0, part
        return owner, block, (y if which == last else 1 - y) * lane, lane

    def pair_copy(which, slot):
        size = place_of(which)[3]
        group = (partner, diagonal)[slot]
        return remote(
            terms.at[which, pl.ds(aligned(group, own), own), pl.ds(0, size)],
            pair_in.at[which, slot, :, pl.ds(0, size)],
            send_sem.at[0],
            pair_recv.at[which, slot],
            {"tp": partner},
        )

    def peer_copy(which):
        size = place_of(which)[3]
        return remote(
            chip_sum.at[which, :, pl.ds(0, size)],
            peer_in.at[which, :, pl.ds(0, size)],
            send_sem.at[1],
            peer_recv.at[which],
            {"tp": across},
        )

    half_depth = hidden.shape[1] // 2

    def weight_of(which, start, size):
        owner, block, _, lanes = place_of(which)
        rows_ = pl.ds(start, size)
        if lanes == part:
            return jnp.concatenate([down_buf[owner, block, half, rows_] for half in range(2)], axis=1)
        return down_buf[owner, block, y if which == last else 1 - y, rows_]

    def half_wait(which, half):
        owner, block = unit_at(min(which, last) - 2)
        wait_of(
            down_buf.at[owner, block, 1 - y, pl.ds(half * half_depth, half_depth)],
            y_down.at[slot_of(owner, z), block * 2 + half],
        )

    def give(which, value):
        terms[which, :, 0 : value.shape[1]] = value.astype(BF16)
        pair_copy(which, 1).start()
        pair_copy(which, 0).start()

    def multiply(which):
        weight = weight_of(which, 0, 2 * half_depth)
        give(which, jnp.dot(hidden[...], weight, preferred_element_type=F32))

    def combine(which):
        size = place_of(which)[3]
        pair_copy(which, 1).wait_recv()
        other = pl.ds(aligned(across, own), own)
        chip_sum[which, :, 0:size] = (
            terms[which, other, 0:size].astype(F32) + pair_in[which, 1, :, 0:size].astype(F32)
        ).astype(BF16)
        peer_copy(which).start()

    def target_of(which):
        owner, block, offset, size = place_of(which)
        return pl.ds(pl.multiple_of(owner * width + block * part + offset, size), size)

    def out_copy(which):
        target = target_of(which)
        return pltpu.make_async_copy(out_buf.at[:, target], out.at[:, target], send_sem.at[2])

    def finish(which):
        size = place_of(which)[3]
        target = target_of(which)
        peer_copy(which).wait_recv()
        pair_copy(which, 0).wait_recv()
        value = (
            terms[which, own_rows, 0:size].astype(F32)
            + pair_in[which, 0, :, 0:size].astype(F32)
            + peer_in[which, :, 0:size].astype(F32)
        )
        out_buf[:, target] = (mixed[:, target] + value).astype(BF16)
        out_copy(which).start()

    forward(46)
    multiply(0)
    forward(47.5)
    multiply(1)
    combine(0)
    forward(49)
    combine(1)
    forward(50)
    for which in range(2, last):
        ready = total + (which - 1) * PIECES
        advance(ready + PIECES, ready + 3 * PIECES)
        half_wait(which, 0)
        half_wait(which, 1)
        multiply(which)
        advance(ready + PIECES * 3 // 2, ready + 3 * PIECES)
        combine(which)
        finish(which - 2)
    multiply(last)
    half_wait(last, 0)
    acc[:, 0:lane] = jnp.dot(
        hidden[:, 0:half_depth],
        weight_of(blocks, 0, half_depth),
        preferred_element_type=F32,
    )
    combine(last)
    finish(last - 2)
    finish(last - 1)
    half_wait(last, 1)
    rest = jnp.dot(
        hidden[:, half_depth:],
        weight_of(blocks, half_depth, half_depth),
        preferred_element_type=F32,
    )
    give(blocks, acc[:, 0:lane] + rest)
    combine(blocks)
    finish(last)
    finish(blocks)

    wait_of(out_buf, send_sem.at[2])
    wait_of(pair_in.at[pl.ds(0, blocks)], send_sem.at[0])
    wait_of(chip_sum.at[pl.ds(0, blocks)], send_sem.at[1])
    wait_of(att_all.at[pl.ds(0, 3)], att_sem.at[0])
    for slot in range(3):
        wait_of(normed.at[own_rows, :], norm_send.at[slot])

    @pl.when(z < n - 1)
    def _():
        wait_of(kv_buf.at[:, :, pl.ds(0, WINDOW)], tail_sem.at[0])

    for weight in range(2):

        @pl.when(is_end)
        def _():
            wait_of(half_of(weight, z, 1 - y), twin_send.at[weight])

        for owner in range(n):

            @pl.when((z >= owner) & (z < n - 1))
            def _():
                wait_of(half_of(weight, owner, y), z_send.at[weight, owner])

            @pl.when((z <= owner) & (z > 0))
            def _():
                wait_of(half_of(weight, owner, y), z_send.at[weight, z_slot(owner, 0)])

            @pl.when((z != owner) & jnp.logical_not(has_twin(owner)))
            def _():
                wait_of(half_of(weight, owner, y), y_send.at[weight, slot_of(owner, z)])


def fused_body(
    n,
    queries,
    key_rows,
    value_rows,
    sink_logits,
    out_weight,
    residual,
    norm_gain,
    up_weight,
    down_weight,
):
    rows, head_cols = queries.shape
    own, wide = residual.shape
    depth, cols = up_weight.shape
    width = down_weight.shape[1]
    part = width // 2
    vmem = lambda *shape: pltpu.VMEM(shape, BF16)
    dma = lambda *shape: pltpu.SemaphoreType.DMA(shape)
    hbm = pl.BlockSpec(memory_space=pl.ANY)
    return pl.pallas_call(
        functools.partial(layer_kernel, n),
        out_shape=pltpu.VMEM((own, wide), BF16),
        in_specs=[
            hbm,
            hbm,
            hbm,
            hbm,
            hbm,
            hbm,
            hbm,
            hbm,
            hbm,
        ],
        out_specs=hbm,
        scratch_shapes=[
            pltpu.SMEM(sink_logits.shape, F32),
            pltpu.VMEM((1, wide), F32),
            vmem(own, wide),
            vmem(rows, head_cols),
            vmem(2, HEAD_DIM, rows + WINDOW),
            vmem(head_cols, rows + WINDOW),
            vmem(head_cols, rows + WINDOW),
            vmem(rows, head_cols),
            vmem(4, own, head_cols),
            vmem(*out_weight.shape),
            vmem(own, wide),
            pltpu.VMEM((own, wide), F32),
            vmem(rows, wide),
            vmem(n * depth, cols),
            vmem(n, 2, 2, cols, part // 2),
            pltpu.VMEM((rows, cols), F32),
            vmem(rows, cols),
            vmem(2 * n + 1, rows, part),
            vmem(2 * n + 1, 2, own, part),
            vmem(2 * n + 1, own, part),
            vmem(2 * n + 1, own, part),
            dma(8),
            dma(2),
            dma(2, n + 1),
            dma(2),
            dma(2, n - 1),
            dma(2, n - 1, CHUNKS),
            dma(n - 1),
            dma(n - 1, 4),
            dma(2),
            dma(3),
            dma(n, 2),
            dma(3),
            dma(2 * n + 1, 2),
            dma(2 * n + 1),
        ],
        compiler_params=pltpu.CompilerParams(
            collective_id=0, has_side_effects=True, vmem_limit_bytes=60 * 1024 * 1024
        ),
    )(
        queries,
        key_rows.T,
        value_rows.T,
        sink_logits,
        out_weight,
        residual,
        norm_gain.reshape(1, -1),
        up_weight,
        down_weight,
    )


def solution(mesh):
    in_specs = (
        P(("grp", "sp"), "tp"),
        P(("grp", "sp"), "tp"),
        P(("grp", "sp"), "tp"),
        P("tp"),
        P(),
        P(("grp", "sp", "tp"), None),
        P(),
        P("sp", "tp"),
        P("tp", "sp"),
    )
    out_specs = P(("grp", "sp", "tp"), None)
    n = mesh.shape["sp"]

    def layer(*arrays):
        key_rows, up_weight, down_weight = arrays[1], arrays[7], arrays[8]
        fits = (
            n == 4
            and mesh.shape["grp"] == 2
            and mesh.shape["tp"] == 4
            and key_rows.shape[1] == HEAD_DIM
            and up_weight.shape[0] % (32 * CHUNKS) == 0
            and up_weight.shape[1] % 256 == 0
            and down_weight.shape[1] % 512 == 0
        )
        return (functools.partial(fused_body, n) if fits else body)(*arrays)

    return jax.shard_map(layer, mesh=mesh, in_specs=in_specs, out_specs=out_specs, check_vma=False)
```

```python
import functools

import jax
import jax.numpy as jnp
from jax import lax
from jax.experimental import pallas as pl
from jax.experimental.pallas import tpu as pltpu
from jax.sharding import PartitionSpec as P

HEAD_DIM = 64
WINDOW = 128


def shifted(value, axis, steps):
    count = lax.axis_size(axis)
    leading, last = (max(0, -steps), min(count, count - steps))
    return lax.ppermute(value, axis, [(source, source + steps) for source in range(leading, last)])


def band_attend(queries, key_rows, value_rows, sink_logits, tail_keys, tail_values, offset):
    rows = queries.shape[0]
    kv_heads = key_rows.shape[1] // HEAD_DIM
    group = queries.shape[1] // (kv_heads * HEAD_DIM)
    blocks = rows // WINDOW
    all_keys = jnp.concatenate([tail_keys, key_rows], axis=0).reshape(
        blocks + 1, WINDOW, kv_heads, HEAD_DIM
    )
    all_values = jnp.concatenate([tail_values, value_rows], axis=0).reshape(
        blocks + 1, WINDOW, kv_heads, HEAD_DIM
    )
    key_blocks = jnp.concatenate([all_keys[:-1], all_keys[1:]], axis=1)
    value_blocks = jnp.concatenate([all_values[:-1], all_values[1:]], axis=1)
    query_blocks = queries.reshape(blocks, WINDOW, kv_heads, group, HEAD_DIM)
    scores = jnp.einsum(
        "nqkgd,nskd->nkgqs", query_blocks, key_blocks, preferred_element_type=jnp.float32
    ) * HEAD_DIM ** (-0.5)
    q_local = jnp.arange(WINDOW, dtype=jnp.int32) + WINDOW
    k_local = jnp.arange(2 * WINDOW, dtype=jnp.int32)
    distance = q_local[:, None] - k_local[None, :]
    key_position = (
        offset + (jnp.arange(blocks, dtype=jnp.int32)[:, None] - 1) * WINDOW + k_local[None, :]
    )
    valid = ((distance >= 0) & (distance < WINDOW))[None] & (key_position >= 0)[:, None, :]
    scores = jnp.where(valid[:, None, None], scores, -1e30)
    sink = sink_logits.reshape(kv_heads, group)[None, :, :, None, None]
    top = jnp.maximum(jnp.max(scores, axis=-1, keepdims=True), sink)
    weights = jnp.exp(scores - top)
    total = jnp.sum(weights, axis=-1, keepdims=True) + jnp.exp(sink - top)
    probs = (weights / total).astype(jnp.bfloat16)
    result = jnp.einsum(
        "nkgqs,nskd->nqkgd", probs, value_blocks, preferred_element_type=jnp.float32
    )
    return result.astype(jnp.bfloat16).reshape(rows, kv_heads * group * HEAD_DIM)


def body(
    queries,
    key_rows,
    value_rows,
    sink_logits,
    out_weight,
    residual,
    norm_gain,
    up_weight,
    down_weight,
):
    rows = queries.shape[0]
    width = key_rows.shape[1]
    kv_pair = jnp.concatenate([key_rows[rows - WINDOW :], value_rows[rows - WINDOW :]], axis=1)
    tail = shifted(kv_pair, "sp", 1)
    offset = lax.axis_index("sp") * rows
    attended = band_attend(
        queries, key_rows, value_rows, sink_logits, tail[:, :width], tail[:, width:], offset
    )
    head_cols = attended.shape[1]
    own_rows = lax.dynamic_slice_in_dim(out_weight, lax.axis_index("tp") * head_cols, head_cols, 0)
    projected = lax.psum_scatter(
        jnp.dot(attended, own_rows, preferred_element_type=jnp.float32).astype(jnp.bfloat16),
        "tp",
        scatter_dimension=0,
        tiled=True,
    ).astype(jnp.float32)
    mixed32 = (residual.astype(jnp.float32) + projected).astype(jnp.bfloat16).astype(jnp.float32)
    scale = lax.rsqrt(jnp.mean(mixed32 * mixed32, axis=-1, keepdims=True) + 1e-06)
    normed = (mixed32 * scale * norm_gain).astype(jnp.bfloat16)
    all_rows = lax.all_gather(normed, "tp", axis=0, tiled=True)
    before = jnp.dot(
        all_rows,
        lax.all_gather(up_weight, "sp", axis=0, tiled=True),
        preferred_element_type=jnp.float32,
    )
    hidden = jnp.square(jax.nn.relu(before)).astype(jnp.bfloat16)
    terms = jnp.dot(
        hidden,
        lax.all_gather(down_weight, "sp", axis=1, tiled=True),
        preferred_element_type=jnp.float32,
    )
    down = lax.psum_scatter(
        terms.astype(jnp.bfloat16), "tp", scatter_dimension=0, tiled=True
    ).astype(jnp.float32)
    return (mixed32 + down).astype(jnp.bfloat16)


PIECES = 4
HOP = 4.7
PACE = 2.8
CHUNKS = 2 * PIECES
F32 = jnp.float32
BF16 = jnp.bfloat16


def remote(src, dst, send_sem, recv_sem, device_id):
    return pltpu.make_async_remote_copy(
        src_ref=src,
        dst_ref=dst,
        send_sem=send_sem,
        recv_sem=recv_sem,
        device_id=device_id,
        device_id_type=pl.DeviceIdType.MESH,
    )


def aligned(value, size):
    return pl.multiple_of(value * size, size)


def layer_kernel(
    n,
    queries,
    keys,
    values,
    sink_in,
    out_weight,
    residual,
    gain_in,
    up,
    down,
    out,
    sink,
    gain,
    out_buf,
    q_buf,
    kv_buf,
    k_wide,
    v_wide,
    attended,
    att_all,
    ow_buf,
    res_buf,
    mixed,
    normed,
    up_buf,
    down_buf,
    acc,
    hidden,
    terms,
    pair_in,
    chip_sum,
    peer_in,
    local_sem,
    tail_sem,
    z_send,
    twin_send,
    y_send,
    z_recv,
    y_up,
    y_down,
    att_sem,
    norm_send,
    norm_recv,
    send_sem,
    pair_recv,
    peer_recv,
):
    z = lax.axis_index("sp")
    y = lax.axis_index("grp")
    me = lax.axis_index("tp")
    partner = me + 1 - 2 * lax.rem(me, 2)
    across = lax.rem(me + 2, 4)
    diagonal = lax.rem(partner + 2, 4)
    rows, head_cols = q_buf.shape
    own = rows // 4
    depth = up.shape[0]
    width = down.shape[1]
    cols = up.shape[1]
    wide = n * width
    part = width // 2
    lane = part // 2
    chunk = (depth // 2 // CHUNKS, down.shape[0] // PIECES)
    near = jnp.minimum(z, n - 1 - z)
    is_end = near == 0
    far_sign = jnp.where(z < n - 1 - z, 1, -1)

    barrier = pltpu.get_barrier_semaphore()
    for step in range(1, 4):
        pl.semaphore_signal(
            barrier,
            inc=1,
            device_id={"tp": lax.rem(me + step, 4)},
            device_id_type=pl.DeviceIdType.MESH,
        )
    pl.semaphore_signal(
        barrier, inc=1, device_id={"grp": 1 - y}, device_id_type=pl.DeviceIdType.MESH
    )

    @pl.when(z > 0)
    def _():
        pl.semaphore_signal(
            barrier, inc=1, device_id={"sp": z - 1}, device_id_type=pl.DeviceIdType.MESH
        )

    @pl.when(z < n - 1)
    def _():
        pl.semaphore_signal(
            barrier, inc=1, device_id={"sp": z + 1}, device_id_type=pl.DeviceIdType.MESH
        )

    own_up = up_buf.at[pl.ds(aligned(z, depth), depth), :]
    wait_of = lambda ref, sem: pltpu.make_async_copy(ref, ref, sem).wait()
    pltpu.make_async_copy(keys, kv_buf.at[0, :, pl.ds(WINDOW, rows)], local_sem.at[0]).start()
    pltpu.make_async_copy(values, kv_buf.at[1, :, pl.ds(WINDOW, rows)], local_sem.at[0]).start()
    for index in range(4):
        source = down.at[:, pl.ds(index * lane, lane)]
        place = down_buf.at[z, index // 2, index % 2]
        pltpu.make_async_copy(source, place, local_sem.at[1]).start()
    locals_ = [
        pltpu.make_async_copy(queries, q_buf, local_sem.at[2]),
        pltpu.make_async_copy(sink_in, sink, local_sem.at[3]),
        pltpu.make_async_copy(out_weight, ow_buf, local_sem.at[4]),
        pltpu.make_async_copy(residual, res_buf, local_sem.at[5]),
        pltpu.make_async_copy(gain_in, gain, local_sem.at[6]),
        pltpu.make_async_copy(up, own_up, local_sem.at[7]),
    ]
    for copy in locals_:
        copy.start()

    edge = jnp.where(z > 0, 1, 0) + jnp.where(z < n - 1, 1, 0)
    pl.semaphore_wait(barrier, 4 + edge)

    def piece(weight, owner, half, index):
        if weight == 0:
            start = owner * depth + half * (depth // 2) + index * chunk[0]
            return up_buf.at[pl.ds(pl.multiple_of(start, chunk[0]), chunk[0]), :]
        return down_buf.at[
            owner, index // PIECES, half, pl.ds(aligned(index % PIECES, chunk[1]), chunk[1]), :
        ]

    def own_piece(weight, half, index):
        if weight == 0:
            start = half * (depth // 2) + index * chunk[0]
            return up.at[pl.ds(pl.multiple_of(start, chunk[0]), chunk[0]), :]
        return piece(weight, z, half, index)

    def half_of(weight, owner, half):
        if weight == 0:
            start = owner * depth + half * (depth // 2)
            return up_buf.at[pl.ds(pl.multiple_of(start, depth // 2), depth // 2), :]
        return down_buf.at[owner, :, half]

    def slot_of(owner, position):
        return lax.rem(owner - position + n, n) - 1

    def z_slot(owner, upward):
        return owner if upward else jnp.where(owner == z, n, owner)

    def z_copy(weight, owner, index, upward, source=None):
        place = piece(weight, owner, y, index)
        target = z + (1 if upward else -1)
        return remote(
            place if source is None else source,
            place,
            z_send.at[weight, z_slot(owner, upward)],
            z_recv.at[weight, slot_of(owner, target), index],
            {"sp": target},
        )

    def half_sem(weight, owner, position, index):
        if weight == 0:
            return y_up.at[slot_of(owner, position)]
        return y_down.at[slot_of(owner, position), index // (PIECES // 2)]

    def twin_copy(weight, index):
        return remote(
            own_piece(weight, 1 - y, index),
            piece(weight, z, 1 - y, index),
            twin_send.at[weight],
            half_sem(weight, z, z + far_sign, index),
            {"sp": z + far_sign},
        )

    def y_copy(weight, owner, index):
        place = piece(weight, owner, y, index)
        return remote(
            place,
            place,
            y_send.at[weight, slot_of(owner, z)],
            half_sem(weight, owner, z, index),
            {"grp": 1 - y},
        )

    def has_twin(owner):
        return ((z == 1) & (owner == 0)) | ((z == n - 2) & (owner == n - 1))

    def each_piece(action):
        def step(index, carry):
            action(index)
            return carry

        lax.fori_loop(0, CHUNKS, step, 0)

    def send_own(weight, upward):
        each_piece(lambda index: z_copy(weight, z, index, upward, own_piece(weight, y, index)).start())

    def tail_copy(which):
        return remote(
            (keys, values)[which].at[:, pl.ds(rows - WINDOW, WINDOW)],
            kv_buf.at[which, :, pl.ds(0, WINDOW)],
            tail_sem.at[0],
            tail_sem.at[1],
            {"sp": z + 1},
        )

    @pl.when((z > 0) & (far_sign > 0))
    def _():
        send_own(0, 0)

    @pl.when(z < n - 1)
    def _():
        tail_copy(0).start()
        tail_copy(1).start()
        send_own(0, 1)

    @pl.when((z > 0) & (far_sign < 0))
    def _():
        send_own(0, 0)

    @pl.when(is_end)
    def _():
        each_piece(lambda index: twin_copy(0, index).start())

    def owner_at(order):
        close = order <= 2 * near
        side = 2 * lax.rem(order + 1, 2) - 1
        return z + jnp.where(close, side * ((order + 1) // 2), far_sign * (order - near))

    def unit_at(unit):
        close = unit < near * 4
        rest = jnp.maximum(unit - near * 4, 0)
        side = 2 * (unit % 2) - 1
        owner = z + jnp.where(
            close, side * (unit // 4 + 1), far_sign * (near + 1 + lax.div(rest, 2))
        )
        return owner, jnp.where(close, (unit % 4) // 2, lax.rem(rest, 2))

    def shard_at(number):
        owner, block = unit_at(number // PIECES)
        return owner, block * PIECES + number % PIECES

    def event(weight, number):
        owner, index = shard_at(number)
        wait_of(piece(weight, owner, y, index), z_recv.at[weight, slot_of(owner, z), index])

        @pl.when((owner < z) & (z < n - 1))
        def _():
            z_copy(weight, owner, index, 1).start()

        @pl.when((owner > z) & (z > 0))
        def _():
            z_copy(weight, owner, index, 0).start()

        skip = has_twin(owner)
        if weight == 1:
            skip |= is_end & (owner == n - 1 - z) & (index // (PIECES // 2) == 3)

        @pl.when(jnp.logical_not(skip))
        def _():
            y_copy(weight, owner, index).start()

    total = (n - 1) * CHUNKS

    def pick(end, middle):
        return end if end == middle else jnp.where(is_end, end, middle)

    arrived = [0, 0]

    def run(weight, goals):
        starts = [min(max(at - weight * total, 0), total) for at in arrived]
        stops = [min(max(at - weight * total, 0), total) for at in goals]
        if starts == stops:
            return

        def step(number, carry):
            event(weight, number)
            return carry

        lax.fori_loop(pick(*starts), pick(*stops), step, 0)

    def advance(end, middle):
        goals = [max(arrived[0], min(end, 2 * total)), max(arrived[1], min(middle, 2 * total))]
        run(0, goals)
        if arrived[1] < total <= goals[1]:

            @pl.when(jnp.logical_not(is_end))
            def _():
                send_own(1, 1)
                send_own(1, 0)

        run(1, goals)
        arrived[:] = goals

    def forward(clock):
        fine = PACE * 4 / CHUNKS
        landed = lambda since: max(int((clock - HOP - since) // fine), 0)
        middle = 0
        for since in (0, 8 * PACE):
            side = min(landed(since), CHUNKS)
            middle += 2 * PIECES * (side // PIECES) + side % PIECES
            middle += min(max(landed(since) - CHUNKS, 0), CHUNKS)
        advance(landed(0), middle)

    @pl.when(z == 0)
    def _():
        kv_buf[:, :, pl.ds(0, WINDOW)] = jnp.zeros((2, HEAD_DIM, WINDOW), BF16)

    wait_of(kv_buf.at[:, :, pl.ds(WINDOW, rows)], local_sem.at[0])
    wait_of(down_buf.at[z], local_sem.at[1])
    for copy in locals_[:2]:
        copy.wait()

    @pl.when(is_end)
    def _():
        @pl.when(z < n - 1)
        def _():
            send_own(1, 1)

        @pl.when(z > 0)
        def _():
            send_own(1, 0)

        each_piece(lambda index: twin_copy(1, index).start())

    @pl.when(z > 0)
    def _():
        wait_of(kv_buf.at[:, :, pl.ds(0, WINDOW)], tail_sem.at[1])

    heads = head_cols // HEAD_DIM
    for h in range(heads):
        k_wide[h * HEAD_DIM : (h + 1) * HEAD_DIM, :] = kv_buf[0]
        v_wide[h * HEAD_DIM : (h + 1) * HEAD_DIM, :] = kv_buf[1]

    def attend(block, carry):
        start = aligned(block, WINDOW)
        q_rows = q_buf[pl.ds(start, WINDOW), :].astype(F32)
        lane_head = lax.broadcasted_iota(jnp.int32, (WINDOW, head_cols), 1) // HEAD_DIM
        stacked = jnp.concatenate(
            [jnp.where(lane_head == h, q_rows, 0.0) for h in range(heads)], axis=0
        ).astype(BF16)
        scores = jnp.dot(
            stacked, k_wide[:, pl.ds(start, 2 * WINDOW)], preferred_element_type=F32
        ) * HEAD_DIM ** (-0.5)
        i = lax.broadcasted_iota(jnp.int32, (heads * WINDOW, 2 * WINDOW), 0) % WINDOW
        j = lax.broadcasted_iota(jnp.int32, (heads * WINDOW, 2 * WINDOW), 1)
        first = WINDOW - z * rows - block * WINDOW
        valid = (j > i) & (j <= i + WINDOW) & (j >= first)
        scores = jnp.where(valid, scores, -1e30)
        sinks = jnp.concatenate(
            [jnp.full((WINDOW, 1), sink[h], F32) for h in range(heads)], axis=0
        )
        top = jnp.maximum(jnp.max(scores, axis=-1, keepdims=True), sinks)
        weights = jnp.exp(scores - top)
        total = jnp.sum(weights, axis=-1, keepdims=True) + jnp.exp(sinks - top)
        probs = (weights / total).astype(BF16)
        mixed_heads = lax.dot_general(
            probs,
            v_wide[:, pl.ds(start, 2 * WINDOW)],
            (((1,), (1,)), ((), ())),
            preferred_element_type=F32,
        )
        result = jnp.zeros((WINDOW, head_cols), F32)
        for h in range(heads):
            result += jnp.where(
                lane_head == h, mixed_heads[h * WINDOW : (h + 1) * WINDOW], 0.0
            )
        attended[pl.ds(start, WINDOW), :] = result.astype(BF16)
        return carry

    blocks = rows // WINDOW
    for block in range(blocks):
        lax.fori_loop(block, block + 1, attend, 0)
        forward(5.5 + 1.35 * block)

    def att_copy(step):
        peer = lax.rem(me + step, 4)
        return remote(
            attended.at[pl.ds(aligned(peer, own), own), :],
            att_all.at[me],
            att_sem.at[0],
            att_sem.at[1],
            {"tp": peer},
        )

    for step in (2, 1, 3):
        att_copy(step).start()
    att_all[me] = attended[pl.ds(aligned(me, own), own), :]
    forward(14.5)
    for copy in locals_[2:5]:
        copy.wait()
    forward(16)
    wait_of(att_all.at[pl.ds(0, 3)], att_sem.at[1])
    forward(18)

    tile = 256

    def project(index, squares):
        span = pl.ds(aligned(index, tile), tile)
        value = res_buf[:, span].astype(F32)
        for peer in range(4):
            value += jnp.dot(
                att_all[peer],
                ow_buf[peer * head_cols : (peer + 1) * head_cols, span],
                preferred_element_type=F32,
            )
        value = value.astype(BF16).astype(F32)
        mixed[:, span] = value
        return squares + jnp.sum(value * value, axis=-1, keepdims=True)

    squares = lax.fori_loop(0, wide // tile // 2, project, jnp.zeros((own, 1), F32))
    forward(19.5)
    squares = lax.fori_loop(wide // tile // 2, wide // tile, project, squares)
    forward(21)
    scale = lax.rsqrt(squares / wide + 1e-06)
    own_rows = pl.ds(aligned(me, own), own)

    def norm_copy(slot, order, source, target):
        place = normed.at[
            pl.ds(aligned(source, own), own), pl.ds(aligned(owner_at(order), depth), depth)
        ]
        link = 0 if slot == 0 else 1
        return remote(place, place, norm_send.at[slot], norm_recv.at[order, link], {"tp": target})

    for order in range(n):
        span = pl.ds(aligned(owner_at(order), depth), depth)
        normed[own_rows, span] = (mixed[:, span] * scale * gain[:, span]).astype(BF16)
        norm_copy(0, order, me, across).start()
        norm_copy(1, order, me, partner).start()

    locals_[5].wait()
    clocks = (29.2, 33.2, 37.4, 41.6)
    for order in range(n):
        owner = owner_at(order)
        forward(clocks[order] - 3)
        forward(clocks[order] - 1.5)
        span = pl.ds(aligned(owner, depth), depth)
        wait_of(normed.at[own_rows, span], norm_recv.at[order, 0])
        norm_copy(2, order, across, partner).start()
        forward(clocks[order])
        if order:
            advance(order * CHUNKS, min(order + order % 2, n - 1) * CHUNKS)
            wait_of(half_of(0, owner, 1 - y), y_up.at[slot_of(owner, z)])
        wait_of(normed.at[pl.ds(0, 2 * own), span], norm_recv.at[order, 1])

        def up_step(index, carry, owner=owner, order=order):
            span = pl.ds(aligned(index, tile), tile)
            value = jnp.dot(
                normed[:, pl.ds(aligned(owner, depth), depth)],
                up_buf[pl.ds(aligned(owner, depth), depth), span],
                preferred_element_type=F32,
            )
            if order:
                value += acc[:, span]
            if order == n - 1:
                hidden[:, span] = jnp.square(jnp.maximum(value, 0.0)).astype(BF16)
            else:
                acc[:, span] = value
            return carry

        lax.fori_loop(0, cols // tile // 2, up_step, 0)
        forward(clocks[order] + 0.6)
        lax.fori_loop(cols // tile // 2, cols // tile, up_step, 0)

    blocks = 2 * n
    last = blocks - 1

    def place_of(which):
        if which < 2:
            return z, which, 0, part
        owner, block = unit_at(min(which, last) - 2)
        if which < last:
            return owner, block, 0, part
        return owner, block, (y if which == last else 1 - y) * lane, lane

    def pair_copy(which, slot):
        size = place_of(which)[3]
        group = (partner, diagonal)[slot]
        return remote(
            terms.at[which, pl.ds(aligned(group, own), own), pl.ds(0, size)],
            pair_in.at[which, slot, :, pl.ds(0, size)],
            send_sem.at[0],
            pair_recv.at[which, slot],
            {"tp": partner},
        )

    def peer_copy(which):
        size = place_of(which)[3]
        return remote(
            chip_sum.at[which, :, pl.ds(0, size)],
            peer_in.at[which, :, pl.ds(0, size)],
            send_sem.at[1],
            peer_recv.at[which],
            {"tp": across},
        )

    half_depth = hidden.shape[1] // 2

    def weight_of(which, start, size):
        owner, block, _, lanes = place_of(which)
        rows_ = pl.ds(start, size)
        if lanes == part:
            return jnp.concatenate([down_buf[owner, block, half, rows_] for half in range(2)], axis=1)
        return down_buf[owner, block, y if which == last else 1 - y, rows_]

    def relay():
        owner, block = unit_at(last - 2)
        place = down_buf.at[owner, block, 1 - y, pl.ds(half_depth, half_depth)]
        return remote(
            place,
            place,
            twin_send.at[2],
            y_down.at[slot_of(owner, z - far_sign), block * 2 + 1],
            {"sp": z - far_sign},
        )

    def half_wait(which, half):
        owner, block = unit_at(min(which, last) - 2)
        wait_of(
            down_buf.at[owner, block, 1 - y, pl.ds(half * half_depth, half_depth)],
            y_down.at[slot_of(owner, z), block * 2 + half],
        )

    def give(which, value):
        terms[which, :, 0 : value.shape[1]] = value.astype(BF16)
        pair_copy(which, 1).start()
        pair_copy(which, 0).start()

    def multiply(which):
        weight = weight_of(which, 0, 2 * half_depth)
        give(which, jnp.dot(hidden[...], weight, preferred_element_type=F32))

    def combine(which):
        size = place_of(which)[3]
        pair_copy(which, 1).wait_recv()
        other = pl.ds(aligned(across, own), own)
        chip_sum[which, :, 0:size] = (
            terms[which, other, 0:size].astype(F32) + pair_in[which, 1, :, 0:size].astype(F32)
        ).astype(BF16)
        peer_copy(which).start()

    def target_of(which):
        owner, block, offset, size = place_of(which)
        return pl.ds(pl.multiple_of(owner * width + block * part + offset, size), size)

    def out_copy(which):
        target = target_of(which)
        return pltpu.make_async_copy(out_buf.at[:, target], out.at[:, target], send_sem.at[2])

    def finish(which):
        size = place_of(which)[3]
        target = target_of(which)
        peer_copy(which).wait_recv()
        pair_copy(which, 0).wait_recv()
        value = (
            terms[which, own_rows, 0:size].astype(F32)
            + pair_in[which, 0, :, 0:size].astype(F32)
            + peer_in[which, :, 0:size].astype(F32)
        )
        out_buf[:, target] = (mixed[:, target] + value).astype(BF16)
        out_copy(which).start()

    forward(46)
    multiply(0)
    forward(47.5)
    multiply(1)
    combine(0)
    forward(49)
    combine(1)
    forward(50)
    def partial(which, half):
        start = half * half_depth
        return jnp.dot(
            hidden[:, start : start + half_depth],
            weight_of(which, start, half_depth),
            preferred_element_type=F32,
        )

    for which in range(2, last):
        ready = total + (which - 1) * PIECES
        final = which == last - 1
        advance(ready + PIECES // (2 if final else 1), ready + 3 * PIECES)
        half_wait(which, 0)
        half_wait(which, 1)
        multiply(which)
        if final:

            @pl.when(jnp.logical_not(is_end))
            def _():
                half_wait(last, 1)
                relay().start()

            break
        advance(ready + PIECES * 3 // 2, ready + 3 * PIECES)
        combine(which)
        finish(which - 2)
    acc[:, 0:lane] = partial(last, 0)
    combine(last - 1)
    advance(2 * total, 2 * total)
    give(last, acc[:, 0:lane] + partial(last, 1))

    @pl.when(is_end)
    def _():
        half_wait(last, 1)

    acc[:, 0:lane] = partial(blocks, 1)
    finish(last - 3)
    combine(last)
    half_wait(last, 0)
    give(blocks, acc[:, 0:lane] + partial(blocks, 0))
    finish(last - 2)
    combine(blocks)
    finish(last - 1)
    finish(last)
    finish(blocks)

    wait_of(out_buf, send_sem.at[2])
    wait_of(pair_in.at[pl.ds(0, blocks)], send_sem.at[0])
    wait_of(chip_sum.at[pl.ds(0, blocks)], send_sem.at[1])
    wait_of(att_all.at[pl.ds(0, 3)], att_sem.at[0])
    for slot in range(3):
        wait_of(normed.at[own_rows, :], norm_send.at[slot])

    @pl.when(z < n - 1)
    def _():
        wait_of(kv_buf.at[:, :, pl.ds(0, WINDOW)], tail_sem.at[0])

    for weight in range(2):

        @pl.when(is_end)
        def _():
            wait_of(half_of(weight, z, 1 - y), twin_send.at[weight])

        if weight == 1:

            @pl.when(jnp.logical_not(is_end))
            def _():
                relay().wait_send()

        for owner in range(n):

            @pl.when((z >= owner) & (z < n - 1))
            def _():
                wait_of(half_of(weight, owner, y), z_send.at[weight, owner])

            @pl.when((z <= owner) & (z > 0))
            def _():
                wait_of(half_of(weight, owner, y), z_send.at[weight, z_slot(owner, 0)])

            short = is_end & (owner == n - 1 - z) & (weight == 1)

            @pl.when((z != owner) & jnp.logical_not(has_twin(owner) | short))
            def _():
                wait_of(half_of(weight, owner, y), y_send.at[weight, slot_of(owner, z)])

            if weight == 1:

                @pl.when(short)
                def _():
                    part_of = up_buf.at[pl.ds(0, 3 * depth // 8), :]
                    wait_of(part_of, y_send.at[weight, slot_of(owner, z)])


def fused_body(
    n,
    queries,
    key_rows,
    value_rows,
    sink_logits,
    out_weight,
    residual,
    norm_gain,
    up_weight,
    down_weight,
):
    rows, head_cols = queries.shape
    own, wide = residual.shape
    depth, cols = up_weight.shape
    width = down_weight.shape[1]
    part = width // 2
    vmem = lambda *shape: pltpu.VMEM(shape, BF16)
    dma = lambda *shape: pltpu.SemaphoreType.DMA(shape)
    hbm = pl.BlockSpec(memory_space=pl.ANY)
    return pl.pallas_call(
        functools.partial(layer_kernel, n),
        out_shape=pltpu.VMEM((own, wide), BF16),
        in_specs=[
            hbm,
            hbm,
            hbm,
            hbm,
            hbm,
            hbm,
            hbm,
            hbm,
            hbm,
        ],
        out_specs=hbm,
        scratch_shapes=[
            pltpu.SMEM(sink_logits.shape, F32),
            pltpu.VMEM((1, wide), F32),
            vmem(own, wide),
            vmem(rows, head_cols),
            vmem(2, HEAD_DIM, rows + WINDOW),
            vmem(head_cols, rows + WINDOW),
            vmem(head_cols, rows + WINDOW),
            vmem(rows, head_cols),
            vmem(4, own, head_cols),
            vmem(*out_weight.shape),
            vmem(own, wide),
            pltpu.VMEM((own, wide), F32),
            vmem(rows, wide),
            vmem(n * depth, cols),
            vmem(n, 2, 2, cols, part // 2),
            pltpu.VMEM((rows, cols), F32),
            vmem(rows, cols),
            vmem(2 * n + 1, rows, part),
            vmem(2 * n + 1, 2, own, part),
            vmem(2 * n + 1, own, part),
            vmem(2 * n + 1, own, part),
            dma(8),
            dma(2),
            dma(2, n + 1),
            dma(3),
            dma(2, n - 1),
            dma(2, n - 1, CHUNKS),
            dma(n - 1),
            dma(n - 1, 4),
            dma(2),
            dma(3),
            dma(n, 2),
            dma(3),
            dma(2 * n + 1, 2),
            dma(2 * n + 1),
        ],
        compiler_params=pltpu.CompilerParams(
            collective_id=0, has_side_effects=True, vmem_limit_bytes=60 * 1024 * 1024
        ),
    )(
        queries,
        key_rows.T,
        value_rows.T,
        sink_logits,
        out_weight,
        residual,
        norm_gain.reshape(1, -1),
        up_weight,
        down_weight,
    )


def solution(mesh):
    in_specs = (
        P(("grp", "sp"), "tp"),
        P(("grp", "sp"), "tp"),
        P(("grp", "sp"), "tp"),
        P("tp"),
        P(),
        P(("grp", "sp", "tp"), None),
        P(),
        P("sp", "tp"),
        P("tp", "sp"),
    )
    out_specs = P(("grp", "sp", "tp"), None)
    n = mesh.shape["sp"]

    def layer(*arrays):
        key_rows, up_weight, down_weight = arrays[1], arrays[7], arrays[8]
        fits = (
            n == 4
            and mesh.shape["grp"] == 2
            and mesh.shape["tp"] == 4
            and key_rows.shape[1] == HEAD_DIM
            and up_weight.shape[0] % (32 * CHUNKS) == 0
            and up_weight.shape[1] % 256 == 0
            and down_weight.shape[1] % 512 == 0
        )
        return (functools.partial(fused_body, n) if fits else body)(*arrays)

    return jax.shard_map(layer, mesh=mesh, in_specs=in_specs, out_specs=out_specs, check_vma=False)
```

```python
import functools

import jax
import jax.numpy as jnp
from jax import lax
from jax.experimental import pallas as pl
from jax.experimental.pallas import tpu as pltpu
from jax.sharding import PartitionSpec as P

HEAD_DIM = 64
WINDOW = 128


def shifted(value, axis, steps):
    count = lax.axis_size(axis)
    leading, last = (max(0, -steps), min(count, count - steps))
    return lax.ppermute(value, axis, [(source, source + steps) for source in range(leading, last)])


def band_attend(queries, key_rows, value_rows, sink_logits, tail_keys, tail_values, offset):
    rows = queries.shape[0]
    kv_heads = key_rows.shape[1] // HEAD_DIM
    group = queries.shape[1] // (kv_heads * HEAD_DIM)
    blocks = rows // WINDOW
    all_keys = jnp.concatenate([tail_keys, key_rows], axis=0).reshape(
        blocks + 1, WINDOW, kv_heads, HEAD_DIM
    )
    all_values = jnp.concatenate([tail_values, value_rows], axis=0).reshape(
        blocks + 1, WINDOW, kv_heads, HEAD_DIM
    )
    key_blocks = jnp.concatenate([all_keys[:-1], all_keys[1:]], axis=1)
    value_blocks = jnp.concatenate([all_values[:-1], all_values[1:]], axis=1)
    query_blocks = queries.reshape(blocks, WINDOW, kv_heads, group, HEAD_DIM)
    scores = jnp.einsum(
        "nqkgd,nskd->nkgqs", query_blocks, key_blocks, preferred_element_type=jnp.float32
    ) * HEAD_DIM ** (-0.5)
    q_local = jnp.arange(WINDOW, dtype=jnp.int32) + WINDOW
    k_local = jnp.arange(2 * WINDOW, dtype=jnp.int32)
    distance = q_local[:, None] - k_local[None, :]
    key_position = (
        offset + (jnp.arange(blocks, dtype=jnp.int32)[:, None] - 1) * WINDOW + k_local[None, :]
    )
    valid = ((distance >= 0) & (distance < WINDOW))[None] & (key_position >= 0)[:, None, :]
    scores = jnp.where(valid[:, None, None], scores, -1e30)
    sink = sink_logits.reshape(kv_heads, group)[None, :, :, None, None]
    top = jnp.maximum(jnp.max(scores, axis=-1, keepdims=True), sink)
    weights = jnp.exp(scores - top)
    total = jnp.sum(weights, axis=-1, keepdims=True) + jnp.exp(sink - top)
    probs = (weights / total).astype(jnp.bfloat16)
    result = jnp.einsum(
        "nkgqs,nskd->nqkgd", probs, value_blocks, preferred_element_type=jnp.float32
    )
    return result.astype(jnp.bfloat16).reshape(rows, kv_heads * group * HEAD_DIM)


def body(
    queries,
    key_rows,
    value_rows,
    sink_logits,
    out_weight,
    residual,
    norm_gain,
    up_weight,
    down_weight,
):
    rows = queries.shape[0]
    width = key_rows.shape[1]
    kv_pair = jnp.concatenate([key_rows[rows - WINDOW :], value_rows[rows - WINDOW :]], axis=1)
    tail = shifted(kv_pair, "sp", 1)
    offset = lax.axis_index("sp") * rows
    attended = band_attend(
        queries, key_rows, value_rows, sink_logits, tail[:, :width], tail[:, width:], offset
    )
    head_cols = attended.shape[1]
    own_rows = lax.dynamic_slice_in_dim(out_weight, lax.axis_index("tp") * head_cols, head_cols, 0)
    projected = lax.psum_scatter(
        jnp.dot(attended, own_rows, preferred_element_type=jnp.float32).astype(jnp.bfloat16),
        "tp",
        scatter_dimension=0,
        tiled=True,
    ).astype(jnp.float32)
    mixed32 = (residual.astype(jnp.float32) + projected).astype(jnp.bfloat16).astype(jnp.float32)
    scale = lax.rsqrt(jnp.mean(mixed32 * mixed32, axis=-1, keepdims=True) + 1e-06)
    normed = (mixed32 * scale * norm_gain).astype(jnp.bfloat16)
    all_rows = lax.all_gather(normed, "tp", axis=0, tiled=True)
    before = jnp.dot(
        all_rows,
        lax.all_gather(up_weight, "sp", axis=0, tiled=True),
        preferred_element_type=jnp.float32,
    )
    hidden = jnp.square(jax.nn.relu(before)).astype(jnp.bfloat16)
    terms = jnp.dot(
        hidden,
        lax.all_gather(down_weight, "sp", axis=1, tiled=True),
        preferred_element_type=jnp.float32,
    )
    down = lax.psum_scatter(
        terms.astype(jnp.bfloat16), "tp", scatter_dimension=0, tiled=True
    ).astype(jnp.float32)
    return (mixed32 + down).astype(jnp.bfloat16)


PIECES = 4
HOP = 4.3
PACE = 2.8
CHUNKS = 2 * PIECES
F32 = jnp.float32
BF16 = jnp.bfloat16


def remote(src, dst, send_sem, recv_sem, device_id):
    return pltpu.make_async_remote_copy(
        src_ref=src,
        dst_ref=dst,
        send_sem=send_sem,
        recv_sem=recv_sem,
        device_id=device_id,
        device_id_type=pl.DeviceIdType.MESH,
    )


def aligned(value, size):
    return pl.multiple_of(value * size, size)


def layer_kernel(
    n,
    queries,
    keys,
    values,
    sink_in,
    out_weight,
    residual,
    gain_in,
    up,
    down,
    out,
    sink,
    gain,
    out_buf,
    q_buf,
    kv_buf,
    k_wide,
    v_wide,
    attended,
    att_all,
    ow_buf,
    res_buf,
    mixed,
    normed,
    up_buf,
    down_buf,
    acc,
    hidden,
    terms,
    pair_in,
    chip_sum,
    peer_in,
    local_sem,
    tail_sem,
    z_send,
    twin_send,
    y_send,
    z_recv,
    y_up,
    y_down,
    att_sem,
    norm_send,
    norm_recv,
    send_sem,
    pair_recv,
    peer_recv,
):
    z = lax.axis_index("sp")
    y = lax.axis_index("grp")
    me = lax.axis_index("tp")
    partner = me + 1 - 2 * lax.rem(me, 2)
    across = lax.rem(me + 2, 4)
    diagonal = lax.rem(partner + 2, 4)
    rows, head_cols = q_buf.shape
    own = rows // 4
    depth = up.shape[0]
    width = down.shape[1]
    cols = up.shape[1]
    wide = n * width
    part = width // 2
    lane = part // 2
    chunk = (depth // 2 // CHUNKS, down.shape[0] // PIECES)
    near = jnp.minimum(z, n - 1 - z)
    is_end = near == 0
    far_sign = jnp.where(z < n - 1 - z, 1, -1)

    barrier = pltpu.get_barrier_semaphore()
    for step in range(1, 4):
        pl.semaphore_signal(
            barrier,
            inc=1,
            device_id={"tp": lax.rem(me + step, 4)},
            device_id_type=pl.DeviceIdType.MESH,
        )
    pl.semaphore_signal(
        barrier, inc=1, device_id={"grp": 1 - y}, device_id_type=pl.DeviceIdType.MESH
    )

    @pl.when(z > 0)
    def _():
        pl.semaphore_signal(
            barrier, inc=1, device_id={"sp": z - 1}, device_id_type=pl.DeviceIdType.MESH
        )

    @pl.when(z < n - 1)
    def _():
        pl.semaphore_signal(
            barrier, inc=1, device_id={"sp": z + 1}, device_id_type=pl.DeviceIdType.MESH
        )

    own_up = up_buf.at[pl.ds(aligned(z, depth), depth), :]
    wait_of = lambda ref, sem: pltpu.make_async_copy(ref, ref, sem).wait()
    pltpu.make_async_copy(keys, kv_buf.at[0, :, pl.ds(WINDOW, rows)], local_sem.at[0]).start()
    pltpu.make_async_copy(values, kv_buf.at[1, :, pl.ds(WINDOW, rows)], local_sem.at[0]).start()
    for index in range(4):
        source = down.at[:, pl.ds(index * lane, lane)]
        place = down_buf.at[z, index // 2, index % 2]
        pltpu.make_async_copy(source, place, local_sem.at[1]).start()
    locals_ = [
        pltpu.make_async_copy(queries, q_buf, local_sem.at[2]),
        pltpu.make_async_copy(sink_in, sink, local_sem.at[3]),
        pltpu.make_async_copy(out_weight, ow_buf, local_sem.at[4]),
        pltpu.make_async_copy(residual, res_buf, local_sem.at[5]),
        pltpu.make_async_copy(gain_in, gain, local_sem.at[6]),
        pltpu.make_async_copy(up, own_up, local_sem.at[7]),
    ]
    for copy in locals_:
        copy.start()

    edge = jnp.where(z > 0, 1, 0) + jnp.where(z < n - 1, 1, 0)
    pl.semaphore_wait(barrier, 4 + edge)

    def piece(weight, owner, half, index):
        if weight == 0:
            start = owner * depth + half * (depth // 2) + index * chunk[0]
            return up_buf.at[pl.ds(pl.multiple_of(start, chunk[0]), chunk[0]), :]
        return down_buf.at[
            owner, index // PIECES, half, pl.ds(aligned(index % PIECES, chunk[1]), chunk[1]), :
        ]

    def own_piece(weight, half, index):
        if weight == 0:
            start = half * (depth // 2) + index * chunk[0]
            return up.at[pl.ds(pl.multiple_of(start, chunk[0]), chunk[0]), :]
        return piece(weight, z, half, index)

    def half_of(weight, owner, half):
        if weight == 0:
            start = owner * depth + half * (depth // 2)
            return up_buf.at[pl.ds(pl.multiple_of(start, depth // 2), depth // 2), :]
        return down_buf.at[owner, :, half]

    def slot_of(owner, position):
        return lax.rem(owner - position + n, n) - 1

    def z_slot(owner, upward):
        return owner if upward else jnp.where(owner == z, n, owner)

    def z_copy(weight, owner, index, upward, source=None):
        place = piece(weight, owner, y, index)
        target = z + (1 if upward else -1)
        return remote(
            place if source is None else source,
            place,
            z_send.at[weight, z_slot(owner, upward)],
            z_recv.at[weight, slot_of(owner, target), index],
            {"sp": target},
        )

    def half_sem(weight, owner, position, index):
        if weight == 0:
            return y_up.at[slot_of(owner, position)]
        return y_down.at[slot_of(owner, position), index // (PIECES // 2)]

    def twin_copy(weight, index):
        return remote(
            own_piece(weight, 1 - y, index),
            piece(weight, z, 1 - y, index),
            twin_send.at[weight],
            half_sem(weight, z, z + far_sign, index),
            {"sp": z + far_sign},
        )

    def y_copy(weight, owner, index):
        place = piece(weight, owner, y, index)
        return remote(
            place,
            place,
            y_send.at[weight, slot_of(owner, z)],
            half_sem(weight, owner, z, index),
            {"grp": 1 - y},
        )

    def has_twin(owner):
        return ((z == 1) & (owner == 0)) | ((z == n - 2) & (owner == n - 1))

    def each_piece(action):
        def step(index, carry):
            action(index)
            return carry

        lax.fori_loop(0, CHUNKS, step, 0)

    def send_own(weight, upward):
        each_piece(lambda index: z_copy(weight, z, index, upward, own_piece(weight, y, index)).start())

    def tail_copy(which):
        return remote(
            (keys, values)[which].at[:, pl.ds(rows - WINDOW, WINDOW)],
            kv_buf.at[which, :, pl.ds(0, WINDOW)],
            tail_sem.at[0],
            tail_sem.at[1],
            {"sp": z + 1},
        )

    @pl.when((z > 0) & (far_sign > 0))
    def _():
        send_own(0, 0)

    @pl.when(z < n - 1)
    def _():
        tail_copy(0).start()
        tail_copy(1).start()
        send_own(0, 1)

    @pl.when((z > 0) & (far_sign < 0))
    def _():
        send_own(0, 0)

    @pl.when(is_end)
    def _():
        each_piece(lambda index: twin_copy(0, index).start())

    def owner_at(order):
        close = order <= 2 * near
        side = 2 * lax.rem(order + 1, 2) - 1
        return z + jnp.where(close, side * ((order + 1) // 2), far_sign * (order - near))

    def unit_at(unit):
        close = unit < near * 4
        rest = jnp.maximum(unit - near * 4, 0)
        side = 2 * (unit % 2) - 1
        owner = z + jnp.where(
            close, side * (unit // 4 + 1), far_sign * (near + 1 + lax.div(rest, 2))
        )
        return owner, jnp.where(close, (unit % 4) // 2, lax.rem(rest, 2))

    def shard_at(number):
        owner, block = unit_at(number // PIECES)
        return owner, block * PIECES + number % PIECES

    def event(weight, number):
        owner, index = shard_at(number)
        wait_of(piece(weight, owner, y, index), z_recv.at[weight, slot_of(owner, z), index])

        @pl.when((owner < z) & (z < n - 1))
        def _():
            z_copy(weight, owner, index, 1).start()

        @pl.when((owner > z) & (z > 0))
        def _():
            z_copy(weight, owner, index, 0).start()

        skip = has_twin(owner)
        if weight == 1:
            skip |= is_end & (owner == n - 1 - z) & (index // (PIECES // 2) == 3)

        @pl.when(jnp.logical_not(skip))
        def _():
            y_copy(weight, owner, index).start()

    total = (n - 1) * CHUNKS

    def pick(end, middle):
        return end if end == middle else jnp.where(is_end, end, middle)

    arrived = [0, 0]

    def run(weight, goals):
        starts = [min(max(at - weight * total, 0), total) for at in arrived]
        stops = [min(max(at - weight * total, 0), total) for at in goals]
        if starts == stops:
            return

        def step(number, carry):
            event(weight, number)
            return carry

        lax.fori_loop(pick(*starts), pick(*stops), step, 0)

    def advance(end, middle):
        goals = [max(arrived[0], min(end, 2 * total)), max(arrived[1], min(middle, 2 * total))]
        run(0, goals)
        if arrived[1] < total <= goals[1]:

            @pl.when(jnp.logical_not(is_end))
            def _():
                send_own(1, 1)
                send_own(1, 0)

        run(1, goals)
        arrived[:] = goals

    def forward(clock):
        fine = PACE * 4 / CHUNKS
        landed = lambda since: max(int((clock - HOP - since) // fine), 0)
        middle = 0
        for since in (0, 8 * PACE):
            side = min(landed(since), CHUNKS)
            middle += 2 * PIECES * (side // PIECES) + side % PIECES
            middle += min(max(landed(since) - CHUNKS, 0), CHUNKS)
        advance(landed(0), middle)

    @pl.when(z == 0)
    def _():
        kv_buf[:, :, pl.ds(0, WINDOW)] = jnp.zeros((2, HEAD_DIM, WINDOW), BF16)

    wait_of(kv_buf.at[:, :, pl.ds(WINDOW, rows)], local_sem.at[0])
    wait_of(down_buf.at[z], local_sem.at[1])
    for copy in locals_[:2]:
        copy.wait()

    @pl.when(is_end)
    def _():
        @pl.when(z < n - 1)
        def _():
            send_own(1, 1)

        @pl.when(z > 0)
        def _():
            send_own(1, 0)

        each_piece(lambda index: twin_copy(1, index).start())

    @pl.when(z > 0)
    def _():
        wait_of(kv_buf.at[:, :, pl.ds(0, WINDOW)], tail_sem.at[1])

    heads = head_cols // HEAD_DIM
    for h in range(heads):
        k_wide[h * HEAD_DIM : (h + 1) * HEAD_DIM, :] = kv_buf[0]
        v_wide[h * HEAD_DIM : (h + 1) * HEAD_DIM, :] = kv_buf[1]

    def attend(block, carry):
        start = aligned(block, WINDOW)
        q_rows = q_buf[pl.ds(start, WINDOW), :].astype(F32)
        lane_head = lax.broadcasted_iota(jnp.int32, (WINDOW, head_cols), 1) // HEAD_DIM
        stacked = jnp.concatenate(
            [jnp.where(lane_head == h, q_rows, 0.0) for h in range(heads)], axis=0
        ).astype(BF16)
        scores = jnp.dot(
            stacked, k_wide[:, pl.ds(start, 2 * WINDOW)], preferred_element_type=F32
        ) * HEAD_DIM ** (-0.5)
        i = lax.broadcasted_iota(jnp.int32, (heads * WINDOW, 2 * WINDOW), 0) % WINDOW
        j = lax.broadcasted_iota(jnp.int32, (heads * WINDOW, 2 * WINDOW), 1)
        first = WINDOW - z * rows - block * WINDOW
        valid = (j > i) & (j <= i + WINDOW) & (j >= first)
        scores = jnp.where(valid, scores, -1e30)
        sinks = jnp.concatenate(
            [jnp.full((WINDOW, 1), sink[h], F32) for h in range(heads)], axis=0
        )
        top = jnp.maximum(jnp.max(scores, axis=-1, keepdims=True), sinks)
        weights = jnp.exp(scores - top)
        total = jnp.sum(weights, axis=-1, keepdims=True) + jnp.exp(sinks - top)
        probs = (weights / total).astype(BF16)
        mixed_heads = lax.dot_general(
            probs,
            v_wide[:, pl.ds(start, 2 * WINDOW)],
            (((1,), (1,)), ((), ())),
            preferred_element_type=F32,
        )
        result = jnp.zeros((WINDOW, head_cols), F32)
        for h in range(heads):
            result += jnp.where(
                lane_head == h, mixed_heads[h * WINDOW : (h + 1) * WINDOW], 0.0
            )
        attended[pl.ds(start, WINDOW), :] = result.astype(BF16)
        return carry

    blocks = rows // WINDOW
    for block in range(blocks):
        lax.fori_loop(block, block + 1, attend, 0)
        forward(5.5 + 1.35 * block)

    def att_copy(step):
        peer = lax.rem(me + step, 4)
        return remote(
            attended.at[pl.ds(aligned(peer, own), own), :],
            att_all.at[me],
            att_sem.at[0],
            att_sem.at[1],
            {"tp": peer},
        )

    for step in (2, 1, 3):
        att_copy(step).start()
    att_all[me] = attended[pl.ds(aligned(me, own), own), :]
    forward(14.5)
    for copy in locals_[2:5]:
        copy.wait()
    forward(16)
    wait_of(att_all.at[pl.ds(0, 3)], att_sem.at[1])
    forward(18)

    tile = 256

    def project(index, squares):
        span = pl.ds(aligned(index, tile), tile)
        value = res_buf[:, span].astype(F32)
        for peer in range(4):
            value += jnp.dot(
                att_all[peer],
                ow_buf[peer * head_cols : (peer + 1) * head_cols, span],
                preferred_element_type=F32,
            )
        value = value.astype(BF16).astype(F32)
        mixed[:, span] = value
        return squares + jnp.sum(value * value, axis=-1, keepdims=True)

    squares = lax.fori_loop(0, wide // tile // 2, project, jnp.zeros((own, 1), F32))
    forward(19.5)
    squares = lax.fori_loop(wide // tile // 2, wide // tile, project, squares)
    forward(21)
    scale = lax.rsqrt(squares / wide + 1e-06)
    own_rows = pl.ds(aligned(me, own), own)

    def norm_copy(slot, order, source, target):
        place = normed.at[
            pl.ds(aligned(source, own), own), pl.ds(aligned(owner_at(order), depth), depth)
        ]
        link = 0 if slot == 0 else 1
        return remote(place, place, norm_send.at[slot], norm_recv.at[order, link], {"tp": target})

    for order in range(n):
        span = pl.ds(aligned(owner_at(order), depth), depth)
        normed[own_rows, span] = (mixed[:, span] * scale * gain[:, span]).astype(BF16)
        norm_copy(0, order, me, across).start()
        norm_copy(1, order, me, partner).start()

    locals_[5].wait()
    clocks = (29.2, 33.2, 37.4, 41.6)
    for order in range(n):
        owner = owner_at(order)
        forward(clocks[order] - 3)
        forward(clocks[order] - 1.5)
        span = pl.ds(aligned(owner, depth), depth)
        wait_of(normed.at[own_rows, span], norm_recv.at[order, 0])
        norm_copy(2, order, across, partner).start()
        forward(clocks[order])
        if order:
            advance(order * CHUNKS, min(order + order % 2, n - 1) * CHUNKS)
            wait_of(half_of(0, owner, 1 - y), y_up.at[slot_of(owner, z)])
        wait_of(normed.at[pl.ds(0, 2 * own), span], norm_recv.at[order, 1])

        def up_step(index, carry, owner=owner, order=order):
            span = pl.ds(aligned(index, tile), tile)
            value = jnp.dot(
                normed[:, pl.ds(aligned(owner, depth), depth)],
                up_buf[pl.ds(aligned(owner, depth), depth), span],
                preferred_element_type=F32,
            )
            if order:
                value += acc[:, span]
            if order == n - 1:
                hidden[:, span] = jnp.square(jnp.maximum(value, 0.0)).astype(BF16)
            else:
                acc[:, span] = value
            return carry

        lax.fori_loop(0, cols // tile // 2, up_step, 0)
        forward(clocks[order] + 0.6)
        lax.fori_loop(cols // tile // 2, cols // tile, up_step, 0)

    blocks = 2 * n
    last = blocks - 1

    def place_of(which):
        if which < 2:
            return z, which, 0, part
        owner, block = unit_at(min(which, last) - 2)
        if which < last:
            return owner, block, 0, part
        return owner, block, (y if which == last else 1 - y) * lane, lane

    def pair_copy(which, slot):
        size = place_of(which)[3]
        group = (partner, diagonal)[slot]
        return remote(
            terms.at[which, pl.ds(aligned(group, own), own), pl.ds(0, size)],
            pair_in.at[which, slot, :, pl.ds(0, size)],
            send_sem.at[0],
            pair_recv.at[which, slot],
            {"tp": partner},
        )

    def peer_copy(which):
        size = place_of(which)[3]
        return remote(
            chip_sum.at[which, :, pl.ds(0, size)],
            peer_in.at[which, :, pl.ds(0, size)],
            send_sem.at[1],
            peer_recv.at[which],
            {"tp": across},
        )

    half_depth = hidden.shape[1] // 2

    def weight_of(which, start, size):
        owner, block, _, lanes = place_of(which)
        rows_ = pl.ds(start, size)
        if lanes == part:
            return jnp.concatenate([down_buf[owner, block, half, rows_] for half in range(2)], axis=1)
        return down_buf[owner, block, y if which == last else 1 - y, rows_]

    def relay():
        owner, block = unit_at(last - 2)
        place = down_buf.at[owner, block, 1 - y, pl.ds(half_depth, half_depth)]
        return remote(
            place,
            place,
            twin_send.at[2],
            y_down.at[slot_of(owner, z - far_sign), block * 2 + 1],
            {"sp": z - far_sign},
        )

    def half_wait(which, half):
        owner, block = unit_at(min(which, last) - 2)
        wait_of(
            down_buf.at[owner, block, 1 - y, pl.ds(half * half_depth, half_depth)],
            y_down.at[slot_of(owner, z), block * 2 + half],
        )

    def give(which, value):
        terms[which, :, 0 : value.shape[1]] = value.astype(BF16)
        pair_copy(which, 1).start()
        pair_copy(which, 0).start()

    def multiply(which):
        weight = weight_of(which, 0, 2 * half_depth)
        give(which, jnp.dot(hidden[...], weight, preferred_element_type=F32))

    def combine(which):
        size = place_of(which)[3]
        pair_copy(which, 1).wait_recv()
        other = pl.ds(aligned(across, own), own)
        chip_sum[which, :, 0:size] = (
            terms[which, other, 0:size].astype(F32) + pair_in[which, 1, :, 0:size].astype(F32)
        ).astype(BF16)
        peer_copy(which).start()

    def target_of(which):
        owner, block, offset, size = place_of(which)
        return pl.ds(pl.multiple_of(owner * width + block * part + offset, size), size)

    def out_copy(which):
        target = target_of(which)
        return pltpu.make_async_copy(out_buf.at[:, target], out.at[:, target], send_sem.at[2])

    def finish(which):
        size = place_of(which)[3]
        target = target_of(which)
        peer_copy(which).wait_recv()
        pair_copy(which, 0).wait_recv()
        value = (
            terms[which, own_rows, 0:size].astype(F32)
            + pair_in[which, 0, :, 0:size].astype(F32)
            + peer_in[which, :, 0:size].astype(F32)
        )
        out_buf[:, target] = (mixed[:, target] + value).astype(BF16)
        out_copy(which).start()

    forward(46)
    multiply(0)
    forward(47.5)
    multiply(1)
    combine(0)
    forward(49)
    combine(1)
    forward(50)
    def partial(which, half):
        start = half * half_depth
        return jnp.dot(
            hidden[:, start : start + half_depth],
            weight_of(which, start, half_depth),
            preferred_element_type=F32,
        )

    for which in range(2, last):
        ready = total + (which - 1) * PIECES
        final = which == last - 1
        advance(ready + PIECES * 3 // 4, ready + 3 * PIECES)
        half_wait(which, 0)
        if final:
            acc[:, lane : lane + part] = partial(which, 0)
        half_wait(which, 1)
        if final:
            give(which, acc[:, lane : lane + part] + partial(which, 1))
        else:
            multiply(which)
        if final:

            @pl.when(jnp.logical_not(is_end))
            def _():
                half_wait(last, 1)
                relay().start()

            break
        advance(ready + PIECES * 3 // 2, ready + 3 * PIECES)
        combine(which)
        finish(which - 2)
    acc[:, 0:lane] = partial(last, 0)
    combine(last - 1)
    advance(2 * total, 2 * total)
    give(last, acc[:, 0:lane] + partial(last, 1))

    @pl.when(is_end)
    def _():
        half_wait(last, 1)

    acc[:, 0:lane] = partial(blocks, 1)
    half_wait(last, 0)
    give(blocks, acc[:, 0:lane] + partial(blocks, 0))
    combine(last)
    finish(last - 3)
    finish(last - 2)
    combine(blocks)
    finish(last - 1)
    finish(last)
    finish(blocks)

    wait_of(out_buf, send_sem.at[2])
    wait_of(pair_in.at[pl.ds(0, blocks)], send_sem.at[0])
    wait_of(chip_sum.at[pl.ds(0, blocks)], send_sem.at[1])
    wait_of(att_all.at[pl.ds(0, 3)], att_sem.at[0])
    for slot in range(3):
        wait_of(normed.at[own_rows, :], norm_send.at[slot])

    @pl.when(z < n - 1)
    def _():
        wait_of(kv_buf.at[:, :, pl.ds(0, WINDOW)], tail_sem.at[0])

    for weight in range(2):

        @pl.when(is_end)
        def _():
            wait_of(half_of(weight, z, 1 - y), twin_send.at[weight])

        if weight == 1:

            @pl.when(jnp.logical_not(is_end))
            def _():
                relay().wait_send()

        for owner in range(n):

            @pl.when((z >= owner) & (z < n - 1))
            def _():
                wait_of(half_of(weight, owner, y), z_send.at[weight, owner])

            @pl.when((z <= owner) & (z > 0))
            def _():
                wait_of(half_of(weight, owner, y), z_send.at[weight, z_slot(owner, 0)])

            short = is_end & (owner == n - 1 - z) & (weight == 1)

            @pl.when((z != owner) & jnp.logical_not(has_twin(owner) | short))
            def _():
                wait_of(half_of(weight, owner, y), y_send.at[weight, slot_of(owner, z)])

            if weight == 1:

                @pl.when(short)
                def _():
                    part_of = up_buf.at[pl.ds(0, 3 * depth // 8), :]
                    wait_of(part_of, y_send.at[weight, slot_of(owner, z)])


def fused_body(
    n,
    queries,
    key_rows,
    value_rows,
    sink_logits,
    out_weight,
    residual,
    norm_gain,
    up_weight,
    down_weight,
):
    rows, head_cols = queries.shape
    own, wide = residual.shape
    depth, cols = up_weight.shape
    width = down_weight.shape[1]
    part = width // 2
    vmem = lambda *shape: pltpu.VMEM(shape, BF16)
    dma = lambda *shape: pltpu.SemaphoreType.DMA(shape)
    hbm = pl.BlockSpec(memory_space=pl.ANY)
    return pl.pallas_call(
        functools.partial(layer_kernel, n),
        out_shape=pltpu.VMEM((own, wide), BF16),
        in_specs=[
            hbm,
            hbm,
            hbm,
            hbm,
            hbm,
            hbm,
            hbm,
            hbm,
            hbm,
        ],
        out_specs=hbm,
        scratch_shapes=[
            pltpu.SMEM(sink_logits.shape, F32),
            pltpu.VMEM((1, wide), F32),
            vmem(own, wide),
            vmem(rows, head_cols),
            vmem(2, HEAD_DIM, rows + WINDOW),
            vmem(head_cols, rows + WINDOW),
            vmem(head_cols, rows + WINDOW),
            vmem(rows, head_cols),
            vmem(4, own, head_cols),
            vmem(*out_weight.shape),
            vmem(own, wide),
            pltpu.VMEM((own, wide), F32),
            vmem(rows, wide),
            vmem(n * depth, cols),
            vmem(n, 2, 2, cols, part // 2),
            pltpu.VMEM((rows, cols), F32),
            vmem(rows, cols),
            vmem(2 * n + 1, rows, part),
            vmem(2 * n + 1, 2, own, part),
            vmem(2 * n + 1, own, part),
            vmem(2 * n + 1, own, part),
            dma(8),
            dma(2),
            dma(2, n + 1),
            dma(3),
            dma(2, n - 1),
            dma(2, n - 1, CHUNKS),
            dma(n - 1),
            dma(n - 1, 4),
            dma(2),
            dma(3),
            dma(n, 2),
            dma(3),
            dma(2 * n + 1, 2),
            dma(2 * n + 1),
        ],
        compiler_params=pltpu.CompilerParams(
            collective_id=0, has_side_effects=True, vmem_limit_bytes=60 * 1024 * 1024
        ),
    )(
        queries,
        key_rows.T,
        value_rows.T,
        sink_logits,
        out_weight,
        residual,
        norm_gain.reshape(1, -1),
        up_weight,
        down_weight,
    )


def solution(mesh):
    in_specs = (
        P(("grp", "sp"), "tp"),
        P(("grp", "sp"), "tp"),
        P(("grp", "sp"), "tp"),
        P("tp"),
        P(),
        P(("grp", "sp", "tp"), None),
        P(),
        P("sp", "tp"),
        P("tp", "sp"),
    )
    out_specs = P(("grp", "sp", "tp"), None)
    n = mesh.shape["sp"]

    def layer(*arrays):
        key_rows, up_weight, down_weight = arrays[1], arrays[7], arrays[8]
        fits = (
            n == 4
            and mesh.shape["grp"] == 2
            and mesh.shape["tp"] == 4
            and key_rows.shape[1] == HEAD_DIM
            and up_weight.shape[0] % (32 * CHUNKS) == 0
            and up_weight.shape[1] % 256 == 0
            and down_weight.shape[1] % 512 == 0
        )
        return (functools.partial(fused_body, n) if fits else body)(*arrays)

    return jax.shard_map(layer, mesh=mesh, in_specs=in_specs, out_specs=out_specs, check_vma=False)
```

```python
import functools

import jax
import jax.numpy as jnp
from jax import lax
from jax.experimental import pallas as pl
from jax.experimental.pallas import tpu as pltpu
from jax.sharding import PartitionSpec as P

HEAD_DIM = 64
WINDOW = 128


def shifted(value, axis, steps):
    count = lax.axis_size(axis)
    leading, last = (max(0, -steps), min(count, count - steps))
    return lax.ppermute(value, axis, [(source, source + steps) for source in range(leading, last)])


def band_attend(queries, key_rows, value_rows, sink_logits, tail_keys, tail_values, offset):
    rows = queries.shape[0]
    kv_heads = key_rows.shape[1] // HEAD_DIM
    group = queries.shape[1] // (kv_heads * HEAD_DIM)
    blocks = rows // WINDOW
    all_keys = jnp.concatenate([tail_keys, key_rows], axis=0).reshape(
        blocks + 1, WINDOW, kv_heads, HEAD_DIM
    )
    all_values = jnp.concatenate([tail_values, value_rows], axis=0).reshape(
        blocks + 1, WINDOW, kv_heads, HEAD_DIM
    )
    key_blocks = jnp.concatenate([all_keys[:-1], all_keys[1:]], axis=1)
    value_blocks = jnp.concatenate([all_values[:-1], all_values[1:]], axis=1)
    query_blocks = queries.reshape(blocks, WINDOW, kv_heads, group, HEAD_DIM)
    scores = jnp.einsum(
        "nqkgd,nskd->nkgqs", query_blocks, key_blocks, preferred_element_type=jnp.float32
    ) * HEAD_DIM ** (-0.5)
    q_local = jnp.arange(WINDOW, dtype=jnp.int32) + WINDOW
    k_local = jnp.arange(2 * WINDOW, dtype=jnp.int32)
    distance = q_local[:, None] - k_local[None, :]
    key_position = (
        offset + (jnp.arange(blocks, dtype=jnp.int32)[:, None] - 1) * WINDOW + k_local[None, :]
    )
    valid = ((distance >= 0) & (distance < WINDOW))[None] & (key_position >= 0)[:, None, :]
    scores = jnp.where(valid[:, None, None], scores, -1e30)
    sink = sink_logits.reshape(kv_heads, group)[None, :, :, None, None]
    top = jnp.maximum(jnp.max(scores, axis=-1, keepdims=True), sink)
    weights = jnp.exp(scores - top)
    total = jnp.sum(weights, axis=-1, keepdims=True) + jnp.exp(sink - top)
    probs = (weights / total).astype(jnp.bfloat16)
    result = jnp.einsum(
        "nkgqs,nskd->nqkgd", probs, value_blocks, preferred_element_type=jnp.float32
    )
    return result.astype(jnp.bfloat16).reshape(rows, kv_heads * group * HEAD_DIM)


def body(
    queries,
    key_rows,
    value_rows,
    sink_logits,
    out_weight,
    residual,
    norm_gain,
    up_weight,
    down_weight,
):
    rows = queries.shape[0]
    width = key_rows.shape[1]
    kv_pair = jnp.concatenate([key_rows[rows - WINDOW :], value_rows[rows - WINDOW :]], axis=1)
    tail = shifted(kv_pair, "sp", 1)
    offset = lax.axis_index("sp") * rows
    attended = band_attend(
        queries, key_rows, value_rows, sink_logits, tail[:, :width], tail[:, width:], offset
    )
    head_cols = attended.shape[1]
    own_rows = lax.dynamic_slice_in_dim(out_weight, lax.axis_index("tp") * head_cols, head_cols, 0)
    projected = lax.psum_scatter(
        jnp.dot(attended, own_rows, preferred_element_type=jnp.float32).astype(jnp.bfloat16),
        "tp",
        scatter_dimension=0,
        tiled=True,
    ).astype(jnp.float32)
    mixed32 = (residual.astype(jnp.float32) + projected).astype(jnp.bfloat16).astype(jnp.float32)
    scale = lax.rsqrt(jnp.mean(mixed32 * mixed32, axis=-1, keepdims=True) + 1e-06)
    normed = (mixed32 * scale * norm_gain).astype(jnp.bfloat16)
    all_rows = lax.all_gather(normed, "tp", axis=0, tiled=True)
    before = jnp.dot(
        all_rows,
        lax.all_gather(up_weight, "sp", axis=0, tiled=True),
        preferred_element_type=jnp.float32,
    )
    hidden = jnp.square(jax.nn.relu(before)).astype(jnp.bfloat16)
    terms = jnp.dot(
        hidden,
        lax.all_gather(down_weight, "sp", axis=1, tiled=True),
        preferred_element_type=jnp.float32,
    )
    down = lax.psum_scatter(
        terms.astype(jnp.bfloat16), "tp", scatter_dimension=0, tiled=True
    ).astype(jnp.float32)
    return (mixed32 + down).astype(jnp.bfloat16)


PIECES = 4
HOP = 4.3
PACE = 2.8
CHUNKS = 2 * PIECES
F32 = jnp.float32
BF16 = jnp.bfloat16


def remote(src, dst, send_sem, recv_sem, device_id):
    return pltpu.make_async_remote_copy(
        src_ref=src,
        dst_ref=dst,
        send_sem=send_sem,
        recv_sem=recv_sem,
        device_id=device_id,
        device_id_type=pl.DeviceIdType.MESH,
    )


def aligned(value, size):
    return pl.multiple_of(value * size, size)


def layer_kernel(
    n,
    queries,
    keys,
    values,
    sink_in,
    out_weight,
    residual,
    gain_in,
    up,
    down,
    out,
    sink,
    gain,
    out_buf,
    q_buf,
    kv_buf,
    k_wide,
    v_wide,
    attended,
    att_all,
    ow_buf,
    res_buf,
    mixed,
    normed,
    up_buf,
    down_buf,
    acc,
    hidden,
    terms,
    pair_in,
    chip_sum,
    peer_in,
    local_sem,
    tail_sem,
    z_send,
    twin_send,
    y_send,
    z_recv,
    y_up,
    y_down,
    att_sem,
    norm_send,
    norm_recv,
    send_sem,
    pair_recv,
    peer_recv,
):
    z = lax.axis_index("sp")
    y = lax.axis_index("grp")
    me = lax.axis_index("tp")
    partner = me + 1 - 2 * lax.rem(me, 2)
    across = lax.rem(me + 2, 4)
    diagonal = lax.rem(partner + 2, 4)
    rows, head_cols = q_buf.shape
    own = rows // 4
    depth = up.shape[0]
    width = down.shape[1]
    cols = up.shape[1]
    wide = n * width
    part = width // 2
    lane = part // 2
    chunk = (depth // 2 // CHUNKS, down.shape[0] // PIECES)
    near = jnp.minimum(z, n - 1 - z)
    is_end = near == 0
    far_sign = jnp.where(z < n - 1 - z, 1, -1)

    barrier = pltpu.get_barrier_semaphore()
    for step in range(1, 4):
        pl.semaphore_signal(
            barrier,
            inc=1,
            device_id={"tp": lax.rem(me + step, 4)},
            device_id_type=pl.DeviceIdType.MESH,
        )
    pl.semaphore_signal(
        barrier, inc=1, device_id={"grp": 1 - y}, device_id_type=pl.DeviceIdType.MESH
    )

    @pl.when(z > 0)
    def _():
        pl.semaphore_signal(
            barrier, inc=1, device_id={"sp": z - 1}, device_id_type=pl.DeviceIdType.MESH
        )

    @pl.when(z < n - 1)
    def _():
        pl.semaphore_signal(
            barrier, inc=1, device_id={"sp": z + 1}, device_id_type=pl.DeviceIdType.MESH
        )

    own_up = up_buf.at[pl.ds(aligned(z, depth), depth), :]
    wait_of = lambda ref, sem: pltpu.make_async_copy(ref, ref, sem).wait()
    pltpu.make_async_copy(keys, kv_buf.at[0, :, pl.ds(WINDOW, rows)], local_sem.at[0]).start()
    pltpu.make_async_copy(values, kv_buf.at[1, :, pl.ds(WINDOW, rows)], local_sem.at[0]).start()
    for index in range(4):
        source = down.at[:, pl.ds(index * lane, lane)]
        place = down_buf.at[z, index // 2, index % 2]
        pltpu.make_async_copy(source, place, local_sem.at[1]).start()
    locals_ = [
        pltpu.make_async_copy(queries, q_buf, local_sem.at[2]),
        pltpu.make_async_copy(sink_in, sink, local_sem.at[3]),
        pltpu.make_async_copy(out_weight, ow_buf, local_sem.at[4]),
        pltpu.make_async_copy(residual, res_buf, local_sem.at[5]),
        pltpu.make_async_copy(gain_in, gain, local_sem.at[6]),
        pltpu.make_async_copy(up, own_up, local_sem.at[7]),
    ]
    for copy in locals_:
        copy.start()

    edge = jnp.where(z > 0, 1, 0) + jnp.where(z < n - 1, 1, 0)
    pl.semaphore_wait(barrier, 4 + edge)

    def piece(weight, owner, half, index):
        if weight == 0:
            start = owner * depth + half * (depth // 2) + index * chunk[0]
            return up_buf.at[pl.ds(pl.multiple_of(start, chunk[0]), chunk[0]), :]
        return down_buf.at[
            owner, index // PIECES, half, pl.ds(aligned(index % PIECES, chunk[1]), chunk[1]), :
        ]

    def own_piece(weight, half, index):
        if weight == 0:
            start = half * (depth // 2) + index * chunk[0]
            return up.at[pl.ds(pl.multiple_of(start, chunk[0]), chunk[0]), :]
        return piece(weight, z, half, index)

    def half_of(weight, owner, half):
        if weight == 0:
            start = owner * depth + half * (depth // 2)
            return up_buf.at[pl.ds(pl.multiple_of(start, depth // 2), depth // 2), :]
        return down_buf.at[owner, :, half]

    def slot_of(owner, position):
        return lax.rem(owner - position + n, n) - 1

    def z_slot(owner, upward):
        return owner if upward else jnp.where(owner == z, n, owner)

    def z_copy(weight, owner, index, upward, source=None):
        place = piece(weight, owner, y, index)
        target = z + (1 if upward else -1)
        return remote(
            place if source is None else source,
            place,
            z_send.at[weight, z_slot(owner, upward)],
            z_recv.at[weight, slot_of(owner, target), index],
            {"sp": target},
        )

    def half_sem(weight, owner, position, index):
        if weight == 0:
            return y_up.at[slot_of(owner, position)]
        return y_down.at[slot_of(owner, position), index // (PIECES // 2)]

    def twin_copy(weight, index):
        return remote(
            own_piece(weight, 1 - y, index),
            piece(weight, z, 1 - y, index),
            twin_send.at[weight],
            half_sem(weight, z, z + far_sign, index),
            {"sp": z + far_sign},
        )

    def y_copy(weight, owner, index):
        place = piece(weight, owner, y, index)
        return remote(
            place,
            place,
            y_send.at[weight, slot_of(owner, z)],
            half_sem(weight, owner, z, index),
            {"grp": 1 - y},
        )

    def has_twin(owner):
        return ((z == 1) & (owner == 0)) | ((z == n - 2) & (owner == n - 1))

    def each_piece(action):
        def step(index, carry):
            action(index)
            return carry

        lax.fori_loop(0, CHUNKS, step, 0)

    def send_own(weight, upward):
        each_piece(lambda index: z_copy(weight, z, index, upward, own_piece(weight, y, index)).start())

    def tail_copy(which):
        return remote(
            (keys, values)[which].at[:, pl.ds(rows - WINDOW, WINDOW)],
            kv_buf.at[which, :, pl.ds(0, WINDOW)],
            tail_sem.at[0],
            tail_sem.at[1],
            {"sp": z + 1},
        )

    @pl.when((z > 0) & (far_sign > 0))
    def _():
        send_own(0, 0)

    @pl.when(z < n - 1)
    def _():
        tail_copy(0).start()
        tail_copy(1).start()
        send_own(0, 1)

    @pl.when((z > 0) & (far_sign < 0))
    def _():
        send_own(0, 0)

    @pl.when(is_end)
    def _():
        each_piece(lambda index: twin_copy(0, index).start())

    def owner_at(order):
        close = order <= 2 * near
        side = 2 * lax.rem(order + 1, 2) - 1
        return z + jnp.where(close, side * ((order + 1) // 2), far_sign * (order - near))

    def unit_at(unit):
        close = unit < near * 4
        rest = jnp.maximum(unit - near * 4, 0)
        side = 2 * (unit % 2) - 1
        owner = z + jnp.where(
            close, side * (unit // 4 + 1), far_sign * (near + 1 + lax.div(rest, 2))
        )
        return owner, jnp.where(close, (unit % 4) // 2, lax.rem(rest, 2))

    def shard_at(number):
        owner, block = unit_at(number // PIECES)
        return owner, block * PIECES + number % PIECES

    def event(weight, number):
        owner, index = shard_at(number)
        wait_of(piece(weight, owner, y, index), z_recv.at[weight, slot_of(owner, z), index])

        @pl.when((owner < z) & (z < n - 1))
        def _():
            z_copy(weight, owner, index, 1).start()

        @pl.when((owner > z) & (z > 0))
        def _():
            z_copy(weight, owner, index, 0).start()

        skip = has_twin(owner)
        if weight == 1:
            skip |= is_end & (owner == n - 1 - z) & (index // (PIECES // 2) == 3)

        @pl.when(jnp.logical_not(skip))
        def _():
            y_copy(weight, owner, index).start()

    total = (n - 1) * CHUNKS

    def pick(end, middle):
        return end if end == middle else jnp.where(is_end, end, middle)

    arrived = [0, 0]

    def run(weight, goals):
        starts = [min(max(at - weight * total, 0), total) for at in arrived]
        stops = [min(max(at - weight * total, 0), total) for at in goals]
        if starts == stops:
            return

        def step(number, carry):
            event(weight, number)
            return carry

        lax.fori_loop(pick(*starts), pick(*stops), step, 0)

    def advance(end, middle):
        goals = [max(arrived[0], min(end, 2 * total)), max(arrived[1], min(middle, 2 * total))]
        run(0, goals)
        if arrived[1] < total <= goals[1]:

            @pl.when(jnp.logical_not(is_end))
            def _():
                send_own(1, 1)
                send_own(1, 0)

        run(1, goals)
        arrived[:] = goals

    def forward(clock):
        fine = PACE * 4 / CHUNKS
        landed = lambda since: max(int((clock - HOP - since) // fine), 0)
        middle = 0
        for since in (0, 8 * PACE):
            side = min(landed(since), CHUNKS)
            middle += 2 * PIECES * (side // PIECES) + side % PIECES
            middle += min(max(landed(since) - CHUNKS, 0), CHUNKS)
        advance(landed(0), middle)

    @pl.when(z == 0)
    def _():
        kv_buf[:, :, pl.ds(0, WINDOW)] = jnp.zeros((2, HEAD_DIM, WINDOW), BF16)

    wait_of(kv_buf.at[:, :, pl.ds(WINDOW, rows)], local_sem.at[0])
    wait_of(down_buf.at[z], local_sem.at[1])
    for copy in locals_[:2]:
        copy.wait()

    @pl.when(is_end)
    def _():
        @pl.when(z < n - 1)
        def _():
            send_own(1, 1)

        @pl.when(z > 0)
        def _():
            send_own(1, 0)

        each_piece(lambda index: twin_copy(1, index).start())

    @pl.when(z > 0)
    def _():
        wait_of(kv_buf.at[:, :, pl.ds(0, WINDOW)], tail_sem.at[1])

    heads = head_cols // HEAD_DIM
    for h in range(heads):
        k_wide[h * HEAD_DIM : (h + 1) * HEAD_DIM, :] = kv_buf[0]
        v_wide[h * HEAD_DIM : (h + 1) * HEAD_DIM, :] = kv_buf[1]

    def attend(block, carry):
        start = aligned(block, WINDOW)
        q_rows = q_buf[pl.ds(start, WINDOW), :].astype(F32)
        lane_head = lax.broadcasted_iota(jnp.int32, (WINDOW, head_cols), 1) // HEAD_DIM
        stacked = jnp.concatenate(
            [jnp.where(lane_head == h, q_rows, 0.0) for h in range(heads)], axis=0
        ).astype(BF16)
        scores = jnp.dot(
            stacked, k_wide[:, pl.ds(start, 2 * WINDOW)], preferred_element_type=F32
        ) * HEAD_DIM ** (-0.5)
        i = lax.broadcasted_iota(jnp.int32, (heads * WINDOW, 2 * WINDOW), 0) % WINDOW
        j = lax.broadcasted_iota(jnp.int32, (heads * WINDOW, 2 * WINDOW), 1)
        first = WINDOW - z * rows - block * WINDOW
        valid = (j > i) & (j <= i + WINDOW) & (j >= first)
        scores = jnp.where(valid, scores, -1e30)
        sinks = jnp.concatenate(
            [jnp.full((WINDOW, 1), sink[h], F32) for h in range(heads)], axis=0
        )
        top = jnp.maximum(jnp.max(scores, axis=-1, keepdims=True), sinks)
        weights = jnp.exp(scores - top)
        total = jnp.sum(weights, axis=-1, keepdims=True) + jnp.exp(sinks - top)
        probs = (weights / total).astype(BF16)
        mixed_heads = lax.dot_general(
            probs,
            v_wide[:, pl.ds(start, 2 * WINDOW)],
            (((1,), (1,)), ((), ())),
            preferred_element_type=F32,
        )
        result = jnp.zeros((WINDOW, head_cols), F32)
        for h in range(heads):
            result += jnp.where(
                lane_head == h, mixed_heads[h * WINDOW : (h + 1) * WINDOW], 0.0
            )
        attended[pl.ds(start, WINDOW), :] = result.astype(BF16)
        return carry

    blocks = rows // WINDOW
    for block in range(blocks):
        lax.fori_loop(block, block + 1, attend, 0)
        forward(5.5 + 1.35 * block)

    def att_copy(step):
        peer = lax.rem(me + step, 4)
        return remote(
            attended.at[pl.ds(aligned(peer, own), own), :],
            att_all.at[me],
            att_sem.at[0],
            att_sem.at[1],
            {"tp": peer},
        )

    for step in (2, 1, 3):
        att_copy(step).start()
    att_all[me] = attended[pl.ds(aligned(me, own), own), :]
    forward(14.5)
    for copy in locals_[2:5]:
        copy.wait()
    forward(16)
    wait_of(att_all.at[pl.ds(0, 3)], att_sem.at[1])
    forward(18)

    tile = 256

    def project(index, squares):
        span = pl.ds(aligned(index, tile), tile)
        value = res_buf[:, span].astype(F32)
        for peer in range(4):
            value += jnp.dot(
                att_all[peer],
                ow_buf[peer * head_cols : (peer + 1) * head_cols, span],
                preferred_element_type=F32,
            )
        value = value.astype(BF16).astype(F32)
        mixed[:, span] = value
        return squares + jnp.sum(value * value, axis=-1, keepdims=True)

    squares = jnp.zeros((own, 1), F32)
    for step in range(4):
        squares = lax.fori_loop(
            step * wide // tile // 4, (step + 1) * wide // tile // 4, project, squares
        )
        forward(18.7 + 0.75 * step)
    scale = lax.rsqrt(squares / wide + 1e-06)
    own_rows = pl.ds(aligned(me, own), own)

    def norm_copy(slot, order, source, target):
        place = normed.at[
            pl.ds(aligned(source, own), own), pl.ds(aligned(owner_at(order), depth), depth)
        ]
        link = 0 if slot == 0 else 1
        return remote(place, place, norm_send.at[slot], norm_recv.at[order, link], {"tp": target})

    for order in range(n):
        span = pl.ds(aligned(owner_at(order), depth), depth)
        normed[own_rows, span] = (mixed[:, span] * scale * gain[:, span]).astype(BF16)
        norm_copy(0, order, me, across).start()
        norm_copy(1, order, me, partner).start()

    locals_[5].wait()
    clocks = (29.2, 33.2, 37.4, 41.6)
    for order in range(n):
        owner = owner_at(order)
        forward(clocks[order] - 3)
        forward(clocks[order] - 1.5)
        span = pl.ds(aligned(owner, depth), depth)
        wait_of(normed.at[own_rows, span], norm_recv.at[order, 0])
        norm_copy(2, order, across, partner).start()
        forward(clocks[order])
        if order:
            advance(order * CHUNKS, min(order + order % 2, n - 1) * CHUNKS)
            wait_of(half_of(0, owner, 1 - y), y_up.at[slot_of(owner, z)])
        wait_of(normed.at[pl.ds(0, 2 * own), span], norm_recv.at[order, 1])

        def up_step(index, carry, owner=owner, order=order):
            span = pl.ds(aligned(index, tile), tile)
            value = jnp.dot(
                normed[:, pl.ds(aligned(owner, depth), depth)],
                up_buf[pl.ds(aligned(owner, depth), depth), span],
                preferred_element_type=F32,
            )
            if order:
                value += acc[:, span]
            if order == n - 1:
                hidden[:, span] = jnp.square(jnp.maximum(value, 0.0)).astype(BF16)
            else:
                acc[:, span] = value
            return carry

        lax.fori_loop(0, cols // tile // 2, up_step, 0)
        forward(clocks[order] + 0.6)
        lax.fori_loop(cols // tile // 2, cols // tile, up_step, 0)

    blocks = 2 * n
    last = blocks - 1

    def place_of(which):
        if which < 2:
            return z, which, 0, part
        owner, block = unit_at(min(which, last) - 2)
        if which < last:
            return owner, block, 0, part
        return owner, block, (y if which == last else 1 - y) * lane, lane

    def pair_copy(which, slot):
        size = place_of(which)[3]
        group = (partner, diagonal)[slot]
        return remote(
            terms.at[which, pl.ds(aligned(group, own), own), pl.ds(0, size)],
            pair_in.at[which, slot, :, pl.ds(0, size)],
            send_sem.at[0],
            pair_recv.at[which],
            {"tp": partner},
        )

    def peer_copy(which):
        size = place_of(which)[3]
        return remote(
            chip_sum.at[which, :, pl.ds(0, size)],
            peer_in.at[which, :, pl.ds(0, size)],
            send_sem.at[1],
            peer_recv.at[which],
            {"tp": across},
        )

    half_depth = hidden.shape[1] // 2

    def weight_of(which, start, size):
        owner, block, _, lanes = place_of(which)
        rows_ = pl.ds(start, size)
        if lanes == part:
            return jnp.concatenate([down_buf[owner, block, half, rows_] for half in range(2)], axis=1)
        return down_buf[owner, block, y if which == last else 1 - y, rows_]

    def relay():
        owner, block = unit_at(last - 2)
        place = down_buf.at[owner, block, 1 - y, pl.ds(half_depth, half_depth)]
        return remote(
            place,
            place,
            twin_send.at[2],
            y_down.at[slot_of(owner, z - far_sign), block * 2 + 1],
            {"sp": z - far_sign},
        )

    def half_wait(which, half):
        owner, block = unit_at(min(which, last) - 2)
        wait_of(
            down_buf.at[owner, block, 1 - y, pl.ds(half * half_depth, half_depth)],
            y_down.at[slot_of(owner, z), block * 2 + half],
        )

    def give(which, value):
        terms[which, :, 0 : value.shape[1]] = value.astype(BF16)
        pair_copy(which, 1).start()
        pair_copy(which, 0).start()

    def multiply(which):
        weight = weight_of(which, 0, 2 * half_depth)
        give(which, jnp.dot(hidden[...], weight, preferred_element_type=F32))

    def combine(which):
        size = place_of(which)[3]
        wait_of(pair_in.at[which, :, :, pl.ds(0, size)], pair_recv.at[which])
        other = pl.ds(aligned(across, own), own)
        chip_sum[which, :, 0:size] = (
            terms[which, other, 0:size].astype(F32) + pair_in[which, 1, :, 0:size].astype(F32)
        ).astype(BF16)
        peer_copy(which).start()

    def target_of(which):
        owner, block, offset, size = place_of(which)
        return pl.ds(pl.multiple_of(owner * width + block * part + offset, size), size)

    def out_copy(which):
        target = target_of(which)
        return pltpu.make_async_copy(out_buf.at[:, target], out.at[:, target], send_sem.at[2])

    def finish(which):
        size = place_of(which)[3]
        target = target_of(which)
        peer_copy(which).wait_recv()
        value = (
            terms[which, own_rows, 0:size].astype(F32)
            + pair_in[which, 0, :, 0:size].astype(F32)
            + peer_in[which, :, 0:size].astype(F32)
        )
        out_buf[:, target] = (mixed[:, target] + value).astype(BF16)
        out_copy(which).start()

    forward(46)
    multiply(0)
    forward(47.5)
    multiply(1)
    combine(0)
    forward(49)
    combine(1)
    forward(50)
    def partial(which, half):
        start = half * half_depth
        return jnp.dot(
            hidden[:, start : start + half_depth],
            weight_of(which, start, half_depth),
            preferred_element_type=F32,
        )

    for which in range(2, last):
        ready = total + (which - 1) * PIECES
        final = which == last - 1
        advance(ready + PIECES * 3 // 4, ready + 3 * PIECES)
        half_wait(which, 0)
        if final:
            acc[:, lane : lane + part] = partial(which, 0)
        half_wait(which, 1)
        if final:
            give(which, acc[:, lane : lane + part] + partial(which, 1))
        else:
            multiply(which)
        if final:

            @pl.when(jnp.logical_not(is_end))
            def _():
                half_wait(last, 1)
                relay().start()

            break
        advance(ready + PIECES * 3 // 2, ready + 3 * PIECES)
        combine(which)
        finish(which - 2)
    acc[:, 0:lane] = partial(last, 0)
    combine(last - 1)
    advance(2 * total, 2 * total)
    give(last, acc[:, 0:lane] + partial(last, 1))

    @pl.when(is_end)
    def _():
        half_wait(last, 1)

    acc[:, 0:lane] = partial(blocks, 1)
    half_wait(last, 0)
    give(blocks, acc[:, 0:lane] + partial(blocks, 0))
    combine(last)
    finish(last - 3)
    finish(last - 2)
    combine(blocks)
    finish(last - 1)
    finish(last)
    finish(blocks)

    wait_of(out_buf, send_sem.at[2])
    wait_of(pair_in.at[pl.ds(0, blocks)], send_sem.at[0])
    wait_of(chip_sum.at[pl.ds(0, blocks)], send_sem.at[1])
    wait_of(att_all.at[pl.ds(0, 3)], att_sem.at[0])
    for slot in range(3):
        wait_of(normed.at[own_rows, :], norm_send.at[slot])

    @pl.when(z < n - 1)
    def _():
        wait_of(kv_buf.at[:, :, pl.ds(0, WINDOW)], tail_sem.at[0])

    for weight in range(2):

        @pl.when(is_end)
        def _():
            wait_of(half_of(weight, z, 1 - y), twin_send.at[weight])

        if weight == 1:

            @pl.when(jnp.logical_not(is_end))
            def _():
                relay().wait_send()

        for owner in range(n):

            @pl.when((z >= owner) & (z < n - 1))
            def _():
                wait_of(half_of(weight, owner, y), z_send.at[weight, owner])

            @pl.when((z <= owner) & (z > 0))
            def _():
                wait_of(half_of(weight, owner, y), z_send.at[weight, z_slot(owner, 0)])

            short = is_end & (owner == n - 1 - z) & (weight == 1)

            @pl.when((z != owner) & jnp.logical_not(has_twin(owner) | short))
            def _():
                wait_of(half_of(weight, owner, y), y_send.at[weight, slot_of(owner, z)])

            if weight == 1:

                @pl.when(short)
                def _():
                    part_of = up_buf.at[pl.ds(0, 3 * depth // 8), :]
                    wait_of(part_of, y_send.at[weight, slot_of(owner, z)])


def fused_body(
    n,
    queries,
    key_rows,
    value_rows,
    sink_logits,
    out_weight,
    residual,
    norm_gain,
    up_weight,
    down_weight,
):
    rows, head_cols = queries.shape
    own, wide = residual.shape
    depth, cols = up_weight.shape
    width = down_weight.shape[1]
    part = width // 2
    vmem = lambda *shape: pltpu.VMEM(shape, BF16)
    dma = lambda *shape: pltpu.SemaphoreType.DMA(shape)
    hbm = pl.BlockSpec(memory_space=pl.ANY)
    return pl.pallas_call(
        functools.partial(layer_kernel, n),
        out_shape=pltpu.VMEM((own, wide), BF16),
        in_specs=[
            hbm,
            hbm,
            hbm,
            hbm,
            hbm,
            hbm,
            hbm,
            hbm,
            hbm,
        ],
        out_specs=hbm,
        scratch_shapes=[
            pltpu.SMEM(sink_logits.shape, F32),
            pltpu.VMEM((1, wide), F32),
            vmem(own, wide),
            vmem(rows, head_cols),
            vmem(2, HEAD_DIM, rows + WINDOW),
            vmem(head_cols, rows + WINDOW),
            vmem(head_cols, rows + WINDOW),
            vmem(rows, head_cols),
            vmem(4, own, head_cols),
            vmem(*out_weight.shape),
            vmem(own, wide),
            pltpu.VMEM((own, wide), F32),
            vmem(rows, wide),
            vmem(n * depth, cols),
            vmem(n, 2, 2, cols, part // 2),
            pltpu.VMEM((rows, cols), F32),
            vmem(rows, cols),
            vmem(2 * n + 1, rows, part),
            vmem(2 * n + 1, 2, own, part),
            vmem(2 * n + 1, own, part),
            vmem(2 * n + 1, own, part),
            dma(8),
            dma(2),
            dma(2, n + 1),
            dma(3),
            dma(2, n - 1),
            dma(2, n - 1, CHUNKS),
            dma(n - 1),
            dma(n - 1, 4),
            dma(2),
            dma(3),
            dma(n, 2),
            dma(3),
            dma(2 * n + 1),
            dma(2 * n + 1),
        ],
        compiler_params=pltpu.CompilerParams(
            collective_id=0, has_side_effects=True, vmem_limit_bytes=60 * 1024 * 1024
        ),
    )(
        queries,
        key_rows.T,
        value_rows.T,
        sink_logits,
        out_weight,
        residual,
        norm_gain.reshape(1, -1),
        up_weight,
        down_weight,
    )


def solution(mesh):
    in_specs = (
        P(("grp", "sp"), "tp"),
        P(("grp", "sp"), "tp"),
        P(("grp", "sp"), "tp"),
        P("tp"),
        P(),
        P(("grp", "sp", "tp"), None),
        P(),
        P("sp", "tp"),
        P("tp", "sp"),
    )
    out_specs = P(("grp", "sp", "tp"), None)
    n = mesh.shape["sp"]

    def layer(*arrays):
        key_rows, up_weight, down_weight = arrays[1], arrays[7], arrays[8]
        fits = (
            n == 4
            and mesh.shape["grp"] == 2
            and mesh.shape["tp"] == 4
            and key_rows.shape[1] == HEAD_DIM
            and up_weight.shape[0] % (32 * CHUNKS) == 0
            and up_weight.shape[1] % 256 == 0
            and down_weight.shape[1] % 512 == 0
        )
        return (functools.partial(fused_body, n) if fits else body)(*arrays)

    return jax.shard_map(layer, mesh=mesh, in_specs=in_specs, out_specs=out_specs, check_vma=False)
```
